32 devices in a mesh: sp: 4 (over z), dp: 8 (over y, x, core).
Axes of the slice: x: 2, y: 2, z: 4, core: 2. Of those that a mesh axis runs over, the one named last changes fastest.
Arguments:
- normed: bfloat16 [8, 512, 2048], P('dp', 'sp'), may hold values from -6 to 6
- values: bfloat16 [8, 512, 2048], P('dp', 'sp'), may hold values from -6 to 6
- gate_in: bfloat16 [8, 512, 2048], P('dp', 'sp'), may hold values from -6 to 6
- step_raw: bfloat16 [8, 512, 32], P('dp', 'sp'), may hold values from -3.5 to 2.5
- upstream: bfloat16 [8, 512, 2048], P('dp', 'sp'), may hold values from -6 to 6
- proj_pair: bfloat16 [2048, 512], P('dp'), may hold values from -0.03125 to 0.03125
- conv_value: float32 [4, 2048], replicated, may hold values from -3 to 3
- conv_pair: float32 [4, 512], replicated, may hold values from -3 to 3
- step_bias: float32 [32], replicated, may hold values from -1 to 1
- decay_log: float32 [32], replicated, may hold values from -12 to -2
- skip: float32 [32], replicated, may hold values from 0.5 to 1.5
Outputs:
- grad_normed: bfloat16 [8, 512, 2048], P('dp', 'sp')
- grad_values: bfloat16 [8, 512, 2048], P('dp', 'sp')
- grad_gate: bfloat16 [8, 512, 2048], P('dp', 'sp')
- grad_step: bfloat16 [8, 512, 32], P('dp', 'sp')
- grad_proj: float32 [2048, 512], P('dp')
The draws below stay inside these ranges and needn't reach their ends.
All inputs are finite; a program needn't handle non-finite values.
Results may differ from the reference program's by a relative error of at most 0.02.
Values may be sent and summed in bfloat16 or wider, within the bound.
A program may use at most 128 MiB of HBM per device.

```python
import math
import jax
import jax.numpy as jnp
from jax import lax

D = 2048
HEADS = 32
HEAD = 64
GROUPS = 2
STATE = 128
TAPS = 4
BLOCK = 64
TOK_DEV = 128
INNER = 2048
LENGTH = 512
BATCH = 8
N_SP = 4


def draw_step_raw(key, part):
    first, second = jax.random.split(jax.random.fold_in(key, 11))
    blocks = LENGTH // TOK_DEV
    shift = jax.random.uniform(first, (BATCH, blocks, 1, HEADS), jnp.float32, -2.0, 1.0)
    noise = jnp.clip(jax.random.normal(second, (BATCH, blocks, TOK_DEV, HEADS), jnp.float32), -3.0, 3.0) * 0.5
    return (shift + noise).reshape(BATCH, LENGTH, HEADS).astype(jnp.bfloat16)


def draw_decay_log(key, part):
    first, second, third = jax.random.split(jax.random.fold_in(key, 23), 3)
    quick_flag = jax.random.randint(first, (HEADS,), 0, 2) == 1
    quick = jnp.exp(jax.random.uniform(second, (HEADS,), jnp.float32, math.log(0.04), math.log(0.12)))
    gentle = jax.random.uniform(third, (HEADS,), jnp.float32, 0.3, 1.0) / LENGTH
    return jnp.log(jnp.where(quick_flag, quick, gentle)).astype(jnp.float32)


def raised(array, own_key, source, target, shards_of, factor):
    def block_of(axis_at):
        return (jnp.arange(array.shape[axis_at]) // (array.shape[axis_at] // shards_of)).reshape((-1,) + (1,) * (array.ndim - 1 - axis_at))

    first = jax.random.permutation(own_key, shards_of)[block_of(target)]
    second = (block_of(target) + shards_of // 2) % shards_of
    return jnp.where((block_of(source) == first) | (block_of(source) == second), factor * array, array)


def block_scale(rng, extent, cuts, least, top_value):
    def one(dim, shards_of):
        heights = jax.random.uniform(jax.random.fold_in(jax.random.fold_in(rng, 6), dim), (shards_of,), jnp.float32, least / len(cuts), top_value / len(cuts))
        return jnp.repeat(jnp.exp(heights), extent[dim] // shards_of).reshape((-1,) + (1,) * (len(extent) - dim - 1))

    level = one(*cuts[0])
    for cut in cuts[1:]:
        level = level * one(*cut)
    return level


def centred(own_key, extent, deviation, bound, pieces=(), kind=jnp.bfloat16):
    loudness = block_scale(own_key, extent, pieces, -0.22, 0.18) if pieces else 1.0
    drawn = jax.random.normal(own_key, extent, jnp.float32) * deviation * loudness
    return jnp.minimum(jnp.maximum(drawn, -bound), bound).astype(kind)


def noise_with(own_key, shape, scale, limit, cuts, heavy, held_as=jnp.bfloat16):
    drawn = scale * jax.random.normal(own_key, shape, jnp.float32)
    if cuts:
        drawn = drawn * block_scale(own_key, shape, cuts, -0.22, 0.18)
    return jnp.clip(raised(drawn, jax.random.fold_in(own_key, 3), *heavy), -limit, limit).astype(held_as)


def setup_inputs(seed: int = 0) -> dict:
    key_list = jax.random.split(jax.random.key(seed), 12)
    normed = noise_with(key_list[0], (BATCH, LENGTH, D), 1.0, 6.0, ((0, 8), (1, 4)), (0, 2, 8, 2.0))
    values = centred(key_list[1], (BATCH, LENGTH, INNER), 1.0, 6.0, ((0, 8), (1, 4)))
    gate_in = centred(key_list[2], (BATCH, LENGTH, INNER), 1.0, 6.0, ((0, 8), (1, 4)))
    step_raw = draw_step_raw(jax.random.fold_in(key_list[11], 71), 0)
    upstream = centred(key_list[4], (BATCH, LENGTH, INNER), 1.0, 6.0, ((0, 8), (1, 4)))
    proj_pair = centred(key_list[5], (D, GROUPS * 2 * STATE), (16 * D) ** -0.5, 0.03125, ((0, 8),))
    conv_value = centred(key_list[6], (TAPS, INNER), TAPS ** -0.5, 3.0, (), jnp.float32)
    conv_pair = centred(key_list[7], (TAPS, GROUPS * 2 * STATE), TAPS ** -0.5, 3.0, (), jnp.float32)
    step_bias = jnp.clip(jax.random.uniform(key_list[8], (HEADS,), jnp.float32, -1.0, 1.0), -1.0, 1.0)
    decay_log = draw_decay_log(jax.random.fold_in(key_list[11], 71), 0)
    skip = jnp.clip(jax.random.uniform(key_list[10], (HEADS,), jnp.float32, 0.5, 1.5), 0.5, 1.5)
    return {"normed": normed, "values": values, "gate_in": gate_in, "step_raw": step_raw, "upstream": upstream, "proj_pair": proj_pair, "conv_value": conv_value, "conv_pair": conv_pair, "step_bias": step_bias, "decay_log": decay_log, "skip": skip}


exact = lax.Precision.HIGHEST

def causal_filter(signal, weights):
    length = signal.shape[0]
    tap_count = weights.shape[0]
    padded = jnp.pad(signal, ((tap_count - 1, 0), (0, 0)))
    summed = jnp.zeros_like(signal)
    for offset in range(tap_count):
        summed = summed + weights[offset] * padded[offset:offset + length]
    return jax.nn.silu(summed)

def silu_slope(gate):
    sig = jax.nn.sigmoid(gate)
    return sig * (1.0 + gate * (1.0 - sig))

def scan_heads(head_value, pair_rows, raw_steps, taps_value, taps_pair, biases, log_rates, skip_gains):
    length, width = head_value.shape
    count = raw_steps.shape[1]
    head_dim = width // count
    state_dim = pair_rows.shape[1] // 2
    blocks = length // BLOCK
    conv_values = causal_filter(head_value, taps_value)
    conv_pairs = causal_filter(pair_rows, taps_pair)
    inject = conv_pairs[:, :state_dim].reshape(blocks, BLOCK, state_dim)
    readout = conv_pairs[:, state_dim:].reshape(blocks, BLOCK, state_dim)
    step_size = jax.nn.softplus(raw_steps + biases[None, :])
    decay_rate = -jnp.exp(log_rates)
    within = jnp.cumsum((step_size * decay_rate[None, :]).reshape(blocks, BLOCK, count), axis=1)
    value_heads = conv_values.reshape(length, count, head_dim)
    scaled = (value_heads * step_size[:, :, None]).reshape(blocks, BLOCK, count, head_dim)
    causal = jnp.tril(jnp.ones((BLOCK, BLOCK), dtype=bool))
    intersect = jnp.einsum('cln,csn->cls', readout, inject, precision=exact)
    spacing = within[:, :, None, :] - within[:, None, :, :]
    weight_diag = jnp.exp(jnp.where(causal[None, :, :, None], spacing, -jnp.inf))
    mixing = intersect[:, :, :, None] * weight_diag
    local_out = jnp.einsum('clsh,cshp->clhp', mixing, scaled, precision=exact)
    to_end = jnp.exp(within[:, -1:, :] - within)
    carried = jnp.einsum('cln,clhp->chpn', inject, scaled * to_end[:, :, :, None], precision=exact)
    block_total = within[:, -1, :]
    running = jnp.cumsum(block_total, axis=0)
    earlier = jnp.tril(jnp.ones((blocks, blocks), dtype=bool), -1)
    link = jnp.exp(jnp.where(earlier[:, :, None], (running - block_total)[:, None, :] - running[None, :, :], -jnp.inf))
    entering = jnp.einsum('cdh,dhpn->chpn', link, carried, precision=exact)
    far_raw = jnp.einsum('cln,chpn->clhp', readout, entering, precision=exact)
    far_out = far_raw * jnp.exp(within)[:, :, :, None]
    direct = (value_heads * skip_gains[None, :, None]).reshape(length, width)
    return (local_out + far_out).reshape(length, width) + direct

def head_grads(head_value, pair_rows, raw_steps, taps_value, taps_pair, biases, log_rates, skip_gains, cotangent):

    def forward(vals, pairs, raws):
        return scan_heads(vals, pairs, raws, taps_value, taps_pair, biases, log_rates, skip_gains)
    output, pullback = jax.vjp(forward, head_value, pair_rows, raw_steps)
    return (output, pullback(cotangent))

def reference(normed, values, gate_in, step_raw, upstream, proj_pair, conv_value, conv_pair, step_bias, decay_log, skip):
    heads_dev = HEADS // N_SP
    width_dev = heads_dev * HEAD
    per_group = N_SP // GROUPS
    pair_width = 2 * STATE
    group_heads = HEADS // GROUPS

    def one_sequence(items):
        token_rows, seq_values, seq_gate, seq_raw, seq_up = items
        pair_pre = jnp.dot(token_rows, proj_pair, preferred_element_type=jnp.float32).astype(jnp.bfloat16)
        gate_float = seq_gate.astype(jnp.float32)
        up_float = seq_up.astype(jnp.float32)
        cot_all = lax.optimization_barrier((up_float * jax.nn.silu(gate_float)).astype(jnp.bfloat16)).astype(jnp.float32)

        def one_device(index):
            first_head = index * heads_dev
            group = first_head // group_heads
            column = first_head * HEAD
            head_value = lax.dynamic_slice_in_dim(seq_values, column, width_dev, 1).astype(jnp.float32)
            pair_rows = lax.dynamic_slice_in_dim(pair_pre, group * pair_width, pair_width, 1).astype(jnp.float32)
            raw_steps = lax.dynamic_slice_in_dim(seq_raw, first_head, heads_dev, 1).astype(jnp.float32)
            taps_value = lax.dynamic_slice_in_dim(conv_value, column, width_dev, 1)
            taps_pair = lax.dynamic_slice_in_dim(conv_pair, group * pair_width, pair_width, 1)
            biases = lax.dynamic_slice_in_dim(step_bias, first_head, heads_dev, 0)
            log_rates = lax.dynamic_slice_in_dim(decay_log, first_head, heads_dev, 0)
            skip_gains = lax.dynamic_slice_in_dim(skip, first_head, heads_dev, 0)
            cotangent = lax.dynamic_slice_in_dim(cot_all, column, width_dev, 1)
            output, grads = head_grads(head_value, pair_rows, raw_steps, taps_value, taps_pair, biases, log_rates, skip_gains, cotangent)
            return (output.astype(jnp.bfloat16), grads[0].astype(jnp.bfloat16), grads[1].astype(jnp.bfloat16), grads[2].astype(jnp.bfloat16))
        outputs, value_grads, pair_grads, step_grads = lax.map(one_device, jnp.arange(N_SP, dtype=jnp.int32))
        side = jnp.moveaxis(outputs, 0, 1).reshape(LENGTH, INNER)
        grad_gate = (up_float * lax.optimization_barrier(side).astype(jnp.float32) * silu_slope(gate_float)).astype(jnp.bfloat16)
        grad_values = jnp.moveaxis(value_grads, 0, 1).reshape(LENGTH, INNER)
        grad_step = jnp.moveaxis(step_grads, 0, 1).reshape(LENGTH, HEADS)
        device_part = lax.optimization_barrier(pair_grads)
        group_sum = device_part.astype(jnp.float32).reshape(GROUPS, per_group, LENGTH, pair_width).sum(axis=1)
        pair_total = jnp.moveaxis(group_sum, 0, 1).reshape(LENGTH, GROUPS * pair_width).astype(jnp.bfloat16)
        grad_normed = lax.dot_general(pair_total, proj_pair, (((1,), (1,)), ((), ())), preferred_element_type=jnp.float32).astype(jnp.bfloat16)
        grad_proj = lax.dot_general(token_rows, pair_total, (((0,), (0,)), ((), ())), preferred_element_type=jnp.float32)
        return (grad_normed, grad_values, grad_gate, grad_step, grad_proj)
    results = lax.map(one_sequence, (normed, values, gate_in, step_raw, upstream))
    return (results[0], results[1], results[2], results[3], lax.optimization_barrier(jnp.sum(results[4], axis=0)))
```

```python
import functools

import jax
import jax.numpy as jnp
from jax import lax
from jax.experimental import pallas as pl
from jax.experimental.pallas import tpu as pltpu
from jax.sharding import PartitionSpec as P

HEAD = 64
STATE = 128
LANES = 128
PAIR = 2 * STATE
EDGE = 16
NEXT = 8
exact = lax.Precision.HIGHEST
f32 = jnp.float32
bf16 = jnp.bfloat16

NN = (((1,), (0,)), ((), ()))
NT = (((1,), (1,)), ((), ()))
TN = (((0,), (0,)), ((), ()))


def mm(a, b, dims):
    return lax.dot_general(a, b, dims, preferred_element_type=f32)


def mm_exact(a, b, dims):
    return lax.dot_general(a, b, dims, precision=exact, preferred_element_type=f32)


def mm_split(a, b, dims):
    high = a.astype(bf16)
    low = (a - high.astype(f32)).astype(bf16)
    return mm(high, b, dims) + mm(low, b, dims)


def silu_parts(s):
    sig = jax.nn.sigmoid(s)
    return s * sig, sig * (1.0 + s * (1.0 - sig))


def mixer_kernel(
    sp,
    dp,
    heads,
    groups,
    chunks,
    normed_in,
    values_in,
    gate_in,
    up_in,
    proj_in,
    step,
    tap_v,
    tap_p,
    bias,
    log_rate,
    skip,
    gn,
    gv,
    gg,
    gs,
    gp,
    nrm,
    val,
    gate,
    up,
    proj,
    nt,
    ntall,
    cot,
    xvb,
    us,
    slv,
    upslope,
    xb,
    xeb,
    edy,
    dec,
    dgs,
    gm,
    pairx,
    bc,
    slp,
    ee,
    car,
    cin,
    cout,
    ybuf,
    dxl,
    zbuf,
    dvb,
    dpb,
    dpair,
    dpall,
    gpl,
    gin,
    gout,
    loc_sem,
    edge_sem,
    pj_send,
    pj_recv,
    pj_relay,
    ch_send,
    ch_recv,
    nx_sem,
    nt_send,
    nt_recv,
    dg_send,
    dg_recv,
    dg_relay,
    gc_send,
    gc_recv,
):
    z = lax.axis_index("sp")
    d = lax.axis_index("dp")
    T = cot.shape[0]
    W = cot.shape[1]
    width = nt.shape[0]
    R = proj_in.shape[0]
    GW = W // groups
    tiles = GW // LANES
    CW = GW // chunks
    nch = dp // 2
    core = lax.rem(d, 2)
    chip = d // 2
    sib = d + 1 - 2 * core
    first = z == 0
    last = z == sp - 1

    def remote(src, dst, ss, rs, to):
        return pltpu.make_async_remote_copy(
            src_ref=src,
            dst_ref=dst,
            send_sem=ss,
            recv_sem=rs,
            device_id=to,
            device_id_type=pl.DeviceIdType.MESH,
        )

    def prow(s):
        return pl.ds(pl.multiple_of(s * R, 16), R)

    def trow(s):
        return pl.ds(pl.multiple_of(s * T, LANES), T)

    def pcol(g):
        return slice(g * PAIR, (g + 1) * PAIR)

    below = lax.max(z - 1, 0)
    above = lax.min(z + 1, sp - 1)

    loads = [
        pltpu.make_async_copy(proj_in, proj.at[prow(d), :], loc_sem.at[0]),
        pltpu.make_async_copy(gate_in, gate, loc_sem.at[1]),
        pltpu.make_async_copy(up_in, up, loc_sem.at[2]),
        pltpu.make_async_copy(values_in, val.at[EDGE : EDGE + T, :], loc_sem.at[3]),
        pltpu.make_async_copy(normed_in, nrm.at[EDGE : EDGE + T, :], loc_sem.at[4]),
    ]
    for load in loads:
        load.start()

    barrier = pltpu.get_barrier_semaphore()
    for off in range(1, dp):
        pl.semaphore_signal(
            barrier,
            inc=1,
            device_id={"dp": lax.rem(d + off, dp)},
            device_id_type=pl.DeviceIdType.MESH,
        )

    @pl.when(z > 0)
    def _():
        pl.semaphore_signal(
            barrier, inc=1, device_id={"sp": below}, device_id_type=pl.DeviceIdType.MESH
        )

    @pl.when(z < sp - 1)
    def _():
        pl.semaphore_signal(
            barrier, inc=1, device_id={"sp": above}, device_id_type=pl.DeviceIdType.MESH
        )

    arrivals = dp - 1 + jnp.where(first, 0, 1) + jnp.where(last, 0, 1)
    pl.semaphore_wait(barrier, arrivals)

    def go_proj(g, s, to, ss):
        at = proj.at[prow(s), pcol(g)]
        return remote(at, at, ss, pj_recv.at[g, s], {"dp": to})

    def chip_peer(off):
        return lax.rem(chip + off, nch) * 2 + core

    def spread_out(go, send):
        for off in range(1, nch):
            to = chip_peer(off)
            go(d, to, send.at[to]).start()
        go(d, sib, send.at[sib]).start()

    def pass_on(go, send, relay):
        for off in range(1, nch):
            s = chip_peer(off)
            go(s, sib, relay.at[s]).wait_recv()
            go(s, sib, relay.at[s]).start()

    def take_rest(go, relay):
        go(sib, sib, relay.at[sib]).wait_recv()
        for off in range(1, nch):
            s = chip_peer(off) + 1 - 2 * core
            go(s, sib, relay.at[s]).wait_recv()

    def drain(go, send, relay):
        for off in range(1, nch):
            to = chip_peer(off)
            go(d, to, send.at[to]).wait_send()
            go(to, sib, relay.at[to]).wait_send()
        go(d, sib, send.at[sib]).wait_send()

    def proj_of(g):
        return lambda s, to, ss: go_proj(g, s, to, ss)

    loads[0].wait()
    spread_out(proj_of(0), pj_send.at[0])

    def go_edge(k):
        src = (values_in, normed_in)[k]
        dst = (val, nrm)[k]
        return remote(
            src.at[T - EDGE : T, :], dst.at[0:EDGE, :], edge_sem.at[0, k], edge_sem.at[1, k], {"sp": above}
        )

    @pl.when(z < sp - 1)
    def _():
        go_edge(0).start()
        go_edge(1).start()

    for g in range(1, groups):
        spread_out(proj_of(g), pj_send.at[g])

    @pl.when(first)
    def _():
        val[0:EDGE, :] = jnp.zeros((EDGE, W), bf16)
        nrm[0:EDGE, :] = jnp.zeros((EDGE, width), bf16)
        cin[0] = jnp.zeros((STATE, W), bf16)
        gin[0] = jnp.zeros(gin.shape[1:], bf16)

    @pl.when(last)
    def _():
        cin[1] = jnp.zeros((STATE, W), bf16)
        gin[1] = jnp.zeros(gin.shape[1:], bf16)
        dvb[:, T : T + NEXT, :] = jnp.zeros((dvb.shape[0], NEXT, LANES), f32)
        dpb[:, T : T + NEXT, :] = jnp.zeros((dpb.shape[0], NEXT, LANES), f32)

    row_i = lax.broadcasted_iota(jnp.int32, (T, T), 0)
    col_i = lax.broadcasted_iota(jnp.int32, (T, T), 1)
    causal = row_i >= col_i
    tri = causal.astype(f32)
    lane = lax.broadcasted_iota(jnp.int32, (T, LANES), 1)
    low = lane < HEAD

    def padded(v):
        return jnp.concatenate([v, jnp.zeros((v.shape[0], LANES - heads), f32)], axis=1)

    def spread(x, j):
        a = x[:, 2 * j : 2 * j + 1]
        b = x[:, 2 * j + 1 : 2 * j + 2]
        mask = low if x.shape[0] == T else low[0 : x.shape[0]]
        return jnp.where(mask, a, b)

    rate = -jnp.exp(padded(log_rate[...]))
    skips = padded(skip[...])
    steps = jnp.concatenate([step[...].astype(f32), jnp.zeros((LANES - heads, T), f32)], axis=0)
    raw = steps.T + padded(bias[...])
    dt = jax.nn.softplus(raw)
    sgs = jax.nn.sigmoid(raw)
    ac = mm_exact(tri, dt * rate, NN)
    ac_t = ac.T
    ea = jnp.exp(ac)
    end = ac[T - 1 : T, :]
    te = jnp.exp(end - ac)
    e_end = jnp.exp(end)

    def halves(v):
        zero = jnp.zeros_like(v)
        return jnp.concatenate([jnp.where(low, v, zero), jnp.where(low, zero, v)], axis=0)

    def conv(buf, k, taps, at):
        total = taps[0:1, at] * buf[k, EDGE - 3 : EDGE - 3 + T, :]
        for i in range(1, 4):
            total = total + taps[i : i + 1, at] * buf[k, EDGE - 3 + i : EDGE - 3 + i + T, :]
        return total

    def conv_back(buf, k, taps, at):
        total = taps[3:4, at] * buf[k, 0:T, :]
        for i in range(3):
            total = total + taps[i : i + 1, at] * buf[k, 3 - i : 3 - i + T, :]
        return total

    def before_pair(g):
        d_g = jnp.zeros((T, T), f32)
        for j in range(g * tiles, (g + 1) * tiles):
            at = slice(j * LANES, (j + 1) * LANES)
            v = gate[:, at].astype(f32)
            upf = up[:, at].astype(f32)
            act, slope = silu_parts(v)
            dy = (upf * act).astype(bf16)
            cot[:, at] = dy
            upslope[:, at] = upf * slope
            xvb[j] = val[:, at].astype(f32)
            u, slope = silu_parts(conv(xvb, j, tap_v, at))
            us[:, at] = u
            slv[:, at] = slope
            x = (u * spread(dt, j)).astype(bf16)
            xb[:, at] = x
            xeb[:, at] = (x.astype(f32) * spread(te, j)).astype(bf16)
            edy[:, at] = (spread(ea, j) * dy.astype(f32)).astype(bf16)
            ee[:, at] = spread(e_end, j)
            d_mix = mm(halves(dy), x, NT)
            for q in range(2):
                h = 2 * j + q
                diff = ac[:, h : h + 1] - ac_t[h : h + 1, :]
                decay = jnp.exp(jnp.where(causal, diff, -1e30))
                dec[h] = decay
                d_g = d_g + d_mix[q * T : (q + 1) * T] * decay
        dgs[g] = d_g.astype(bf16)

    def pair_stage(g):
        lanes = slice(g * GW, (g + 1) * GW)
        pb = mm(nrm[...], proj[:, pcol(g)], NN).astype(bf16).astype(f32)
        for i in range(2):
            k = 2 * g + i
            at = slice(k * LANES, (k + 1) * LANES)
            pairx[k] = pb[:, i * LANES : (i + 1) * LANES]
            act, slope = silu_parts(conv(pairx, k, tap_p, at))
            bc[k] = act.astype(bf16)
            slp[k] = slope
        b = bc[2 * g]
        cc = bc[2 * g + 1]
        gm[g] = mm(cc, b, NT)
        car[0, :, lanes] = mm(b, xeb[:, lanes], TN)
        car[1, :, lanes] = mm(cc, edy[:, lanes], TN)

    def local_mix(g):
        gmat = gm[g]
        for j in range(g * tiles, (g + 1) * tiles):
            at = slice(j * LANES, (j + 1) * LANES)
            mixes = [(gmat * dec[2 * j + q]).astype(bf16) for q in range(2)]
            ybuf[:, at] = mm(jnp.concatenate(mixes, axis=1), halves(xb[:, at]), NN)
            dxl[:, at] = mm(jnp.concatenate(mixes, axis=0), halves(cot[:, at]), TN)

    def has_in(q):
        return jnp.where(q == 0, z > 0, z < sp - 1)

    def has_out(q):
        return jnp.where(q == 0, z < sp - 1, z > 0)

    def onward(q):
        return lax.max(lax.min(z + 1 - 2 * q, sp - 1), 0)

    def go_state(q, i):
        lanes = slice(i * CW, (i + 1) * CW)
        return remote(
            cout.at[q, :, lanes], cin.at[q, :, lanes], ch_send.at[q, i], ch_recv.at[q, i], {"sp": onward(q)}
        )

    def chain(q, g):
        for i in range(g * chunks, (g + 1) * chunks):
            lanes = slice(i * CW, (i + 1) * CW)

            @pl.when(has_in(q))
            def _():
                go_state(q, i).wait_recv()

            @pl.when(has_out(q))
            def _():
                total = cin[q, :, lanes].astype(f32) * ee[0:1, lanes] + car[q, :, lanes]
                cout[q, :, lanes] = total.astype(bf16)
                go_state(q, i).start()

    early = jnp.where(z < sp // 2, 0, 1)
    late = 1 - early
    at_end = (z == 0) | (z == sp - 1)

    def go_next(kind, g):
        buf = (dpb, dvb)[kind]
        n = (2, tiles)[kind]
        part = buf.at[g * n : (g + 1) * n]
        return remote(
            part.at[:, 0:NEXT, :],
            part.at[:, T : T + NEXT, :],
            nx_sem.at[0, kind, g],
            nx_sem.at[1, kind, g],
            {"sp": below},
        )

    def send_next(kind, g):
        @pl.when(z > 0)
        def _():
            go_next(kind, g).start()

    def take_next(kind, g):
        @pl.when(z < sp - 1)
        def _():
            go_next(kind, g).wait_recv()

    def pair_grads(g):
        lanes = slice(g * GW, (g + 1) * GW)
        b = bc[2 * g]
        cc = bc[2 * g + 1]
        dg = dgs[g]
        d_b = mm(dg, cc, TN) + mm(xeb[:, lanes], cin[1, :, lanes], NT)
        d_c = mm(dg, b, NN) + mm(edy[:, lanes], cin[0, :, lanes], NT)
        dpb[2 * g, 0:T, :] = d_b * slp[2 * g]
        dpb[2 * g + 1, 0:T, :] = d_c * slp[2 * g + 1]
        send_next(0, g)

    def go_dpair(g):
        def go(s, to, ss):
            at = dpall.at[trow(s), pcol(g)]
            return remote(at, at, ss, dg_recv.at[g, s], {"dp": to})

        return go

    def pair_back(g):
        take_next(0, g)
        for i in range(2):
            k = 2 * g + i
            at = slice(k * LANES, (k + 1) * LANES)
            grad = conv_back(dpb, k, tap_p, at).astype(bf16)
            dpair[:, at] = grad
            dpall[trow(d), at] = grad
        spread_out(go_dpair(g), dg_send.at[g])

    def value_grads(g):
        b = bc[2 * g]
        cc = bc[2 * g + 1]
        for j in range(g * tiles, (g + 1) * tiles):
            at = slice(j * LANES, (j + 1) * LANES)
            s_in = cin[0, :, at]
            ds = cin[1, :, at]
            dyf = cot[:, at].astype(f32)
            u = us[:, at]
            y = ybuf[:, at] + spread(ea, j) * mm(cc, s_in, NN)
            zbuf[0, 0:T, at] = dyf * y
            ybf = (y + spread(skips, j) * u).astype(bf16)
            gg[:, at] = (upslope[:, at] * ybf.astype(f32)).astype(bf16)
            x = xb[:, at].astype(f32)
            tej = spread(te, j)
            far = mm(b, ds, NN)
            dx = dxl[:, at] + tej * far
            zbuf[1, 0:T, at] = x * dx
            ends = jnp.sum(x * tej * far, axis=0, keepdims=True) + ee[:, at] * jnp.sum(
                ds.astype(f32) * s_in.astype(f32), axis=0, keepdims=True
            )
            zbuf[1, T : T + NEXT, at] = jnp.broadcast_to(ends, (NEXT, LANES))
            du = spread(dt, j) * dx + spread(skips, j) * dyf
            dvb[j, 0:T, :] = du * slv[:, at]
        send_next(1, g)

    def value_back(g):
        take_next(1, g)
        for j in range(g * tiles, (g + 1) * tiles):
            at = slice(j * LANES, (j + 1) * LANES)
            gv[:, at] = conv_back(dvb, j, tap_v, at).astype(bf16)

    def step_grads():
        sel_r = lax.broadcasted_iota(jnp.int32, (LANES, W), 0)
        sel_c = lax.broadcasted_iota(jnp.int32, (LANES, W), 1)
        sel = jnp.where(sel_c // HEAD == sel_r, 1.0, 0.0).astype(bf16)
        r1 = mm_split(zbuf[0, 0:T, :], sel, NT)
        both = mm_split(zbuf[1], sel, NT)
        xd = both[0:T]
        d_end = both[T : T + 1]
        back = mm_exact(tri, r1 - xd, TN) + d_end
        d_dt = (xd / dt + rate * back) * sgs
        gs[...] = d_dt.T[0:heads, :].astype(bf16)

    def go_nt(to):
        return remote(
            nt.at[prow(to), :], ntall.at[:, trow(d)], nt_send.at[to], nt_recv.at[d], {"dp": to}
        )

    def nt_from(s):
        return remote(nt.at[prow(d), :], ntall.at[:, trow(s)], nt_send.at[s], nt_recv.at[s], {"dp": s})

    def send_normed():
        for k in range(width // LANES):
            at = slice(k * LANES, (k + 1) * LANES)
            nt[at, :] = nrm[EDGE : EDGE + T, at].T
        for off in range(1, dp):
            go_nt(lax.rem(d + off, dp)).start()
        ntall[:, trow(d)] = nt[prow(d), :]

    def go_rows(q, k):
        lanes = slice(k * LANES, (k + 1) * LANES)
        return remote(
            gout.at[q, :, lanes], gin.at[q, :, lanes], gc_send.at[q, k], gc_recv.at[q, k], {"sp": onward(q)}
        )

    def rows_step(q, k):
        lanes = slice(k * LANES, (k + 1) * LANES)

        @pl.when(has_in(q))
        def _():
            go_rows(q, k).wait_recv()

        @pl.when(has_out(q))
        def _():
            gout[q, :, lanes] = (gin[q, :, lanes].astype(f32) + gpl[:, lanes]).astype(bf16)
            go_rows(q, k).start()

    def rows_product(g):
        take_rest(go_dpair(g), dg_relay.at[g])
        gpl[:, pcol(g)] = mm(ntall[...], dpall[:, pcol(g)], NN)

    def rows_total(k):
        lanes = slice(k * LANES, (k + 1) * LANES)
        gp[:, lanes] = gin[0, :, lanes].astype(f32) + gpl[:, lanes] + gin[1, :, lanes].astype(f32)

    loads[1].wait()
    loads[2].wait()
    loads[3].wait()

    @pl.when(z > 0)
    def _():
        go_edge(0).wait_recv()

    before_pair(0)
    pass_on(proj_of(0), pj_send.at[0], pj_relay.at[0])
    for g in range(1, groups):
        before_pair(g)
    loads[4].wait()

    @pl.when(z > 0)
    def _():
        go_edge(1).wait_recv()

    for g in range(groups):
        if g > 0:
            pass_on(proj_of(g), pj_send.at[g], pj_relay.at[g])
        take_rest(proj_of(g), pj_relay.at[g])
        pair_stage(g)

        @pl.when(at_end)
        def _():
            chain(early, g)

        local_mix(g)
        if g == 0:
            send_normed()

    for g in range(groups):
        @pl.when(jnp.logical_not(at_end))
        def _():
            chain(early, g)

        chain(late, g)
        pair_grads(g)
        if g > 0:
            value_grads(g - 1)
        pair_back(g)
    value_grads(groups - 1)
    for g in range(groups):
        pass_on(go_dpair(g), dg_send.at[g], dg_relay.at[g])
    for s in range(1, dp):
        nt_from(lax.rem(d + s, dp)).wait_recv()
    for g in range(groups):
        rows_product(g)
        for k in range(2 * g, 2 * g + 2):
            @pl.when(at_end)
            def _():
                rows_step(early, k)

    for k in range(2 * groups):
        @pl.when(jnp.logical_not(at_end))
        def _():
            rows_step(early, k)

    for k in range(width // 512):
        at = slice(k * 512, (k + 1) * 512)
        gn[:, at] = mm(dpair[...], proj[at, :], NT).astype(bf16)
    for g in range(groups):
        value_back(g)
    step_grads()
    for k in range(2 * groups):
        rows_step(late, k)
        rows_total(k)

    for g in range(groups):
        drain(proj_of(g), pj_send.at[g], pj_relay.at[g])
        drain(go_dpair(g), dg_send.at[g], dg_relay.at[g])
    for off in range(1, dp):
        go_nt(lax.rem(d + off, dp)).wait_send()

    @pl.when(z < sp - 1)
    def _():
        go_edge(0).wait_send()
        go_edge(1).wait_send()

    @pl.when(z > 0)
    def _():
        for g in range(groups):
            go_next(0, g).wait_send()
            go_next(1, g).wait_send()

    for q in range(2):
        @pl.when(has_out(q))
        def _():
            for i in range(groups * chunks):
                go_state(q, i).wait_send()
            for k in range(2 * groups):
                go_rows(q, k).wait_send()


def per_device(
    normed,
    values,
    gate_in,
    step_raw,
    upstream,
    proj_pair,
    conv_value,
    conv_pair,
    step_bias,
    decay_log,
    skip,
):
    sp = lax.axis_size("sp")
    dp = lax.axis_size("dp")
    T = normed.shape[1]
    width = normed.shape[2]
    W = values.shape[2]
    heads = step_raw.shape[2]
    cols = proj_pair.shape[1]
    groups = cols // PAIR
    R = proj_pair.shape[0]
    chunks = 4
    vmem = pl.BlockSpec(memory_space=pltpu.VMEM)
    anyspace = pl.BlockSpec(memory_space=pl.ANY)
    V = pltpu.VMEM
    dma = pltpu.SemaphoreType.DMA
    vt = W // LANES
    pt = cols // LANES
    scratch = [
        V((EDGE + T, width), bf16),
        V((EDGE + T, W), bf16),
        V((T, W), bf16),
        V((T, W), bf16),
        V((width, cols), bf16),
        V((width, T), bf16),
        V((R, dp * T), bf16),
        V((T, W), bf16),
        V((vt, EDGE + T, LANES), f32),
        V((T, W), f32),
        V((T, W), f32),
        V((T, W), f32),
        V((T, W), bf16),
        V((T, W), bf16),
        V((T, W), bf16),
        V((heads, T, T), f32),
        V((groups, T, T), bf16),
        V((groups, T, T), f32),
        V((pt, EDGE + T, LANES), f32),
        V((pt, T, LANES), bf16),
        V((pt, T, LANES), f32),
        V((1, W), f32),
        V((2, STATE, W), f32),
        V((2, STATE, W), bf16),
        V((2, STATE, W), bf16),
        V((T, W), f32),
        V((T, W), f32),
        V((2, T + NEXT, W), f32),
        V((vt, T + NEXT, LANES), f32),
        V((pt, T + NEXT, LANES), f32),
        V((T, cols), bf16),
        V((dp * T, cols), bf16),
        V((R, cols), f32),
        V((2, R, cols), bf16),
        V((2, R, cols), bf16),
        dma((5,)),
        dma((2, 2)),
        dma((groups, dp)),
        dma((groups, dp)),
        dma((groups, dp)),
        dma((2, groups * chunks)),
        dma((2, groups * chunks)),
        dma((2, 2, groups)),
        dma((dp,)),
        dma((dp,)),
        dma((groups, dp)),
        dma((groups, dp)),
        dma((groups, dp)),
        dma((2, pt)),
        dma((2, pt)),
    ]
    gn, gv, gg, gs, gp = pl.pallas_call(
        functools.partial(mixer_kernel, sp, dp, heads, groups, chunks),
        out_shape=(
            jax.ShapeDtypeStruct((T, width), bf16),
            jax.ShapeDtypeStruct((T, W), bf16),
            jax.ShapeDtypeStruct((T, W), bf16),
            jax.ShapeDtypeStruct((heads, T), bf16),
            jax.ShapeDtypeStruct((R, cols), f32),
        ),
        in_specs=[anyspace] * 5 + [vmem] * 6,
        out_specs=(vmem,) * 5,
        scratch_shapes=scratch,
        compiler_params=pltpu.CompilerParams(
            collective_id=0, has_side_effects=True, vmem_limit_bytes=56 * 1024 * 1024
        ),
    )(
        normed[0],
        values[0],
        gate_in[0],
        upstream[0],
        proj_pair,
        step_raw[0].T,
        conv_value,
        conv_pair,
        step_bias[None],
        decay_log[None],
        skip[None],
    )
    return (gn[None], gv[None], gg[None], gs.T[None], gp)


def solution(mesh):
    tok = P("dp", "sp", None)
    in_specs = (tok, tok, tok, tok, tok, P("dp", None), P(), P(), P(), P(), P())
    out_specs = (tok, tok, tok, tok, P("dp", None))
    return jax.shard_map(
        per_device, mesh=mesh, in_specs=in_specs, out_specs=out_specs, check_vma=False
    )
```

```python
import functools

import jax
import jax.numpy as jnp
from jax import lax
from jax.experimental import pallas as pl
from jax.experimental.pallas import tpu as pltpu
from jax.sharding import PartitionSpec as P

HEAD = 64
STATE = 128
LANES = 128
PAIR = 2 * STATE
EDGE = 16
NEXT = 8
exact = lax.Precision.HIGHEST
f32 = jnp.float32
bf16 = jnp.bfloat16

NN = (((1,), (0,)), ((), ()))
NT = (((1,), (1,)), ((), ()))
TN = (((0,), (0,)), ((), ()))


def mm(a, b, dims):
    return lax.dot_general(a, b, dims, preferred_element_type=f32)


def mm_exact(a, b, dims):
    return lax.dot_general(a, b, dims, precision=exact, preferred_element_type=f32)


def mm_split(a, b, dims):
    high = a.astype(bf16)
    low = (a - high.astype(f32)).astype(bf16)
    return mm(high, b, dims) + mm(low, b, dims)


def silu_parts(s):
    sig = jax.nn.sigmoid(s)
    return s * sig, sig * (1.0 + s * (1.0 - sig))


def mixer_kernel(
    sp,
    dp,
    heads,
    groups,
    chunks,
    cuts,
    normed_in,
    values_in,
    gate_in,
    up_in,
    proj_in,
    step_in,
    tap_v_in,
    tap_p_in,
    bias_in,
    log_rate_in,
    skip_in,
    gn,
    gv,
    gg,
    gs,
    gp,
    step,
    tap_v,
    tap_p,
    bias,
    log_rate,
    skip,
    nrm,
    val,
    gate,
    up,
    proj,
    nt,
    ntall,
    cot,
    xvb,
    us,
    slv,
    upslope,
    xb,
    xeb,
    edy,
    dec,
    dgs,
    gm,
    pairx,
    bc,
    slp,
    ee,
    car,
    cin,
    cout,
    ybuf,
    dxl,
    zbuf,
    dvb,
    dpb,
    dpair,
    dpall,
    gpl,
    gin,
    gout,
    loc_sem,
    edge_sem,
    pj_send,
    pj_recv,
    pj_relay,
    ch_send,
    ch_recv,
    nx_sem,
    nt_send,
    nt_recv,
    dg_send,
    dg_recv,
    dg_relay,
    gc_send,
    gc_recv,
):
    z = lax.axis_index("sp")
    d = lax.axis_index("dp")
    T = cot.shape[0]
    W = cot.shape[1]
    width = nt.shape[0]
    R = proj_in.shape[0]
    GW = W // groups
    tiles = GW // LANES
    CW = GW // chunks
    nch = dp // 2
    core = lax.rem(d, 2)
    chip = d // 2
    sib = d + 1 - 2 * core
    first = z == 0
    last = z == sp - 1

    def remote(src, dst, ss, rs, to):
        return pltpu.make_async_remote_copy(
            src_ref=src,
            dst_ref=dst,
            send_sem=ss,
            recv_sem=rs,
            device_id=to,
            device_id_type=pl.DeviceIdType.MESH,
        )

    def prow(s):
        return pl.ds(pl.multiple_of(s * R, 16), R)

    def trow(s):
        return pl.ds(pl.multiple_of(s * T, LANES), T)

    def pcol(g):
        return slice(g * PAIR, (g + 1) * PAIR)

    below = lax.max(z - 1, 0)
    above = lax.min(z + 1, sp - 1)

    loads = [
        pltpu.make_async_copy(proj_in, proj.at[prow(d), :], loc_sem.at[0]),
        pltpu.make_async_copy(gate_in, gate, loc_sem.at[1]),
        pltpu.make_async_copy(up_in, up, loc_sem.at[2]),
        pltpu.make_async_copy(values_in, val.at[EDGE : EDGE + T, :], loc_sem.at[3]),
        pltpu.make_async_copy(normed_in, nrm.at[EDGE : EDGE + T, :], loc_sem.at[4]),
    ]
    small = [
        pltpu.make_async_copy(src, dst, loc_sem.at[5 + k])
        for k, (src, dst) in enumerate(
            (
                (step_in, step),
                (bias_in, bias),
                (log_rate_in, log_rate),
                (skip_in, skip),
                (tap_v_in, tap_v),
                (tap_p_in, tap_p),
            )
        )
    ]
    loads[0].start()
    for load in small + loads[1:]:
        load.start()

    barrier = pltpu.get_barrier_semaphore()
    for off in range(1, dp):
        pl.semaphore_signal(
            barrier,
            inc=1,
            device_id={"dp": lax.rem(d + off, dp)},
            device_id_type=pl.DeviceIdType.MESH,
        )

    @pl.when(z > 0)
    def _():
        pl.semaphore_signal(
            barrier, inc=1, device_id={"sp": below}, device_id_type=pl.DeviceIdType.MESH
        )

    @pl.when(z < sp - 1)
    def _():
        pl.semaphore_signal(
            barrier, inc=1, device_id={"sp": above}, device_id_type=pl.DeviceIdType.MESH
        )

    arrivals = dp - 1 + jnp.where(first, 0, 1) + jnp.where(last, 0, 1)
    pl.semaphore_wait(barrier, arrivals)

    def go_proj(g, s, to, ss):
        at = proj.at[prow(s), pcol(g)]
        return remote(at, at, ss, pj_recv.at[g, s], {"dp": to})

    def chip_peer(off):
        return lax.rem(chip + off, nch) * 2 + core

    def spread_out(go, send):
        for off in range(1, nch):
            to = chip_peer(off)
            go(d, to, send.at[to]).start()
        go(d, sib, send.at[sib]).start()

    def pass_on(go, send, relay):
        for off in range(1, nch):
            s = chip_peer(off)
            go(s, sib, relay.at[s]).wait_recv()
            go(s, sib, relay.at[s]).start()

    def take_rest(go, relay):
        go(sib, sib, relay.at[sib]).wait_recv()
        for off in range(1, nch):
            s = chip_peer(off) + 1 - 2 * core
            go(s, sib, relay.at[s]).wait_recv()

    def drain(go, send, relay):
        for off in range(1, nch):
            to = chip_peer(off)
            go(d, to, send.at[to]).wait_send()
            go(to, sib, relay.at[to]).wait_send()
        go(d, sib, send.at[sib]).wait_send()

    def proj_of(g):
        return lambda s, to, ss: go_proj(g, s, to, ss)

    loads[0].wait()
    spread_out(proj_of(0), pj_send.at[0])

    def go_edge(k):
        src = (values_in, normed_in)[k]
        dst = (val, nrm)[k]
        return remote(
            src.at[T - EDGE : T, :], dst.at[0:EDGE, :], edge_sem.at[0, k], edge_sem.at[1, k], {"sp": above}
        )

    @pl.when(z < sp - 1)
    def _():
        go_edge(0).start()
        go_edge(1).start()

    for g in range(1, groups):
        spread_out(proj_of(g), pj_send.at[g])

    @pl.when(first)
    def _():
        val[0:EDGE, :] = jnp.zeros((EDGE, W), bf16)
        nrm[0:EDGE, :] = jnp.zeros((EDGE, width), bf16)
        cin[0] = jnp.zeros((STATE, W), bf16)
        gin[0] = jnp.zeros(gin.shape[1:], bf16)

    @pl.when(last)
    def _():
        cin[1] = jnp.zeros((STATE, W), bf16)
        gin[1] = jnp.zeros(gin.shape[1:], bf16)
        dvb[:, T : T + NEXT, :] = jnp.zeros((dvb.shape[0], NEXT, LANES), f32)
        dpb[:, T : T + NEXT, :] = jnp.zeros((dpb.shape[0], NEXT, LANES), f32)

    for load in small:
        load.wait()
    row_i = lax.broadcasted_iota(jnp.int32, (T, T), 0)
    col_i = lax.broadcasted_iota(jnp.int32, (T, T), 1)
    causal = row_i >= col_i
    tri = causal.astype(f32)
    lane = lax.broadcasted_iota(jnp.int32, (T, LANES), 1)
    low = lane < HEAD

    def padded(v):
        return jnp.concatenate([v, jnp.zeros((v.shape[0], LANES - heads), f32)], axis=1)

    def spread(x, j):
        a = x[:, 2 * j : 2 * j + 1]
        b = x[:, 2 * j + 1 : 2 * j + 2]
        mask = low if x.shape[0] == T else low[0 : x.shape[0]]
        return jnp.where(mask, a, b)

    rate = -jnp.exp(padded(log_rate[...]))
    skips = padded(skip[...])
    steps = jnp.concatenate([step[...].astype(f32), jnp.zeros((LANES - heads, T), f32)], axis=0)
    raw = steps.T + padded(bias[...])
    dt = jax.nn.softplus(raw)
    sgs = jax.nn.sigmoid(raw)
    ac = mm_exact(tri, dt * rate, NN)
    ac_t = ac.T
    ea = jnp.exp(ac)
    end = ac[T - 1 : T, :]
    te = jnp.exp(end - ac)
    e_end = jnp.exp(end)

    def halves(v):
        zero = jnp.zeros_like(v)
        return jnp.concatenate([jnp.where(low, v, zero), jnp.where(low, zero, v)], axis=0)

    def conv(buf, k, taps, at):
        total = taps[0:1, at] * buf[k, EDGE - 3 : EDGE - 3 + T, :]
        for i in range(1, 4):
            total = total + taps[i : i + 1, at] * buf[k, EDGE - 3 + i : EDGE - 3 + i + T, :]
        return total

    def conv_back(buf, k, taps, at):
        total = taps[3:4, at] * buf[k, 0:T, :]
        for i in range(3):
            total = total + taps[i : i + 1, at] * buf[k, 3 - i : 3 - i + T, :]
        return total

    def before_pair(g):
        d_g = jnp.zeros((T, T), f32)
        for j in range(g * tiles, (g + 1) * tiles):
            at = slice(j * LANES, (j + 1) * LANES)
            v = gate[:, at].astype(f32)
            upf = up[:, at].astype(f32)
            act, slope = silu_parts(v)
            dy = (upf * act).astype(bf16)
            cot[:, at] = dy
            upslope[:, at] = upf * slope
            xvb[j] = val[:, at].astype(f32)
            u, slope = silu_parts(conv(xvb, j, tap_v, at))
            us[:, at] = u
            slv[:, at] = slope
            x = (u * spread(dt, j)).astype(bf16)
            xb[:, at] = x
            xeb[:, at] = (x.astype(f32) * spread(te, j)).astype(bf16)
            edy[:, at] = (spread(ea, j) * dy.astype(f32)).astype(bf16)
            ee[:, at] = spread(e_end, j)
            d_mix = mm(halves(dy), x, NT)
            for q in range(2):
                h = 2 * j + q
                diff = ac[:, h : h + 1] - ac_t[h : h + 1, :]
                decay = jnp.exp(jnp.where(causal, diff, -1e30))
                dec[h] = decay
                d_g = d_g + d_mix[q * T : (q + 1) * T] * decay
        dgs[g] = d_g.astype(bf16)

    def pair_stage(g):
        lanes = slice(g * GW, (g + 1) * GW)
        pb = mm(nrm[...], proj[:, pcol(g)], NN).astype(bf16).astype(f32)
        for i in range(2):
            k = 2 * g + i
            at = slice(k * LANES, (k + 1) * LANES)
            pairx[k] = pb[:, i * LANES : (i + 1) * LANES]
            act, slope = silu_parts(conv(pairx, k, tap_p, at))
            bc[k] = act.astype(bf16)
            slp[k] = slope
        b = bc[2 * g]
        cc = bc[2 * g + 1]
        gm[g] = mm(cc, b, NT)
        car[0, :, lanes] = mm(b, xeb[:, lanes], TN)
        car[1, :, lanes] = mm(cc, edy[:, lanes], TN)

    def local_mix(g):
        gmat = gm[g]
        for j in range(g * tiles, (g + 1) * tiles):
            at = slice(j * LANES, (j + 1) * LANES)
            mixes = [(gmat * dec[2 * j + q]).astype(bf16) for q in range(2)]
            ybuf[:, at] = mm(jnp.concatenate(mixes, axis=1), halves(xb[:, at]), NN)
            dxl[:, at] = mm(jnp.concatenate(mixes, axis=0), halves(cot[:, at]), TN)

    def has_in(q):
        return jnp.where(q == 0, z > 0, z < sp - 1)

    def has_out(q):
        return jnp.where(q == 0, z < sp - 1, z > 0)

    def onward(q):
        return lax.max(lax.min(z + 1 - 2 * q, sp - 1), 0)

    def go_state(q, i):
        lanes = slice(i * CW, (i + 1) * CW)
        return remote(
            cout.at[q, :, lanes], cin.at[q, :, lanes], ch_send.at[q, i], ch_recv.at[q, i], {"sp": onward(q)}
        )

    def chain_step(q, i):
        lanes = slice(i * CW, (i + 1) * CW)

        @pl.when(has_in(q))
        def _():
            go_state(q, i).wait_recv()

        @pl.when(has_out(q))
        def _():
            total = cin[q, :, lanes].astype(f32) * ee[0:1, lanes] + car[q, :, lanes]
            cout[q, :, lanes] = total.astype(bf16)
            go_state(q, i).start()

    def chain_ends(g):
        @pl.when(at_end)
        def _():
            for i in range(g * chunks, (g + 1) * chunks):
                chain_step(early, i)

    def chain_early(i):
        @pl.when(jnp.logical_not(at_end))
        def _():
            chain_step(early, i)

    early = jnp.where(z < sp // 2, 0, 1)
    late = 1 - early
    at_end = (z == 0) | (z == sp - 1)

    def go_next(kind, g):
        buf = (dpb, dvb)[kind]
        n = (2, tiles)[kind]
        part = buf.at[g * n : (g + 1) * n]
        return remote(
            part.at[:, 0:NEXT, :],
            part.at[:, T : T + NEXT, :],
            nx_sem.at[0, kind, g],
            nx_sem.at[1, kind, g],
            {"sp": below},
        )

    def send_next(kind, g):
        @pl.when(z > 0)
        def _():
            go_next(kind, g).start()

    def take_next(kind, g):
        @pl.when(z < sp - 1)
        def _():
            go_next(kind, g).wait_recv()

    def pair_grads(g):
        lanes = slice(g * GW, (g + 1) * GW)
        b = bc[2 * g]
        cc = bc[2 * g + 1]
        dg = dgs[g]
        d_b = mm(dg, cc, TN) + mm(xeb[:, lanes], cin[1, :, lanes], NT)
        d_c = mm(dg, b, NN) + mm(edy[:, lanes], cin[0, :, lanes], NT)
        dpb[2 * g, 0:T, :] = d_b * slp[2 * g]
        dpb[2 * g + 1, 0:T, :] = d_c * slp[2 * g + 1]
        send_next(0, g)

    def go_dpair(g):
        def go(s, to, ss):
            at = dpall.at[trow(s), pcol(g)]
            return remote(at, at, ss, dg_recv.at[g, s], {"dp": to})

        return go

    def pair_back(g):
        take_next(0, g)
        for i in range(2):
            k = 2 * g + i
            at = slice(k * LANES, (k + 1) * LANES)
            grad = conv_back(dpb, k, tap_p, at).astype(bf16)
            dpair[:, at] = grad
            dpall[trow(d), at] = grad
        spread_out(go_dpair(g), dg_send.at[g])

    def value_grads(g):
        b = bc[2 * g]
        cc = bc[2 * g + 1]
        for j in range(g * tiles, (g + 1) * tiles):
            at = slice(j * LANES, (j + 1) * LANES)
            s_in = cin[0, :, at]
            ds = cin[1, :, at]
            dyf = cot[:, at].astype(f32)
            u = us[:, at]
            y = ybuf[:, at] + spread(ea, j) * mm(cc, s_in, NN)
            zbuf[0, 0:T, at] = dyf * y
            ybf = (y + spread(skips, j) * u).astype(bf16)
            gg[:, at] = (upslope[:, at] * ybf.astype(f32)).astype(bf16)
            x = xb[:, at].astype(f32)
            tej = spread(te, j)
            far = mm(b, ds, NN)
            dx = dxl[:, at] + tej * far
            zbuf[1, 0:T, at] = x * dx
            ends = jnp.sum(x * tej * far, axis=0, keepdims=True) + ee[:, at] * jnp.sum(
                ds.astype(f32) * s_in.astype(f32), axis=0, keepdims=True
            )
            zbuf[1, T : T + NEXT, at] = jnp.broadcast_to(ends, (NEXT, LANES))
            du = spread(dt, j) * dx + spread(skips, j) * dyf
            dvb[j, 0:T, :] = du * slv[:, at]
        send_next(1, g)

    def value_back(g):
        take_next(1, g)
        for j in range(g * tiles, (g + 1) * tiles):
            at = slice(j * LANES, (j + 1) * LANES)
            gv[:, at] = conv_back(dvb, j, tap_v, at).astype(bf16)

    def step_grads():
        sel_r = lax.broadcasted_iota(jnp.int32, (LANES, W), 0)
        sel_c = lax.broadcasted_iota(jnp.int32, (LANES, W), 1)
        sel = jnp.where(sel_c // HEAD == sel_r, 1.0, 0.0).astype(bf16)
        r1 = mm_split(zbuf[0, 0:T, :], sel, NT)
        both = mm_split(zbuf[1], sel, NT)
        xd = both[0:T]
        d_end = both[T : T + 1]
        back = mm_exact(tri, r1 - xd, TN) + d_end
        d_dt = (xd / dt + rate * back) * sgs
        gs[...] = d_dt.T[0:heads, :].astype(bf16)

    def go_nt(to):
        return remote(
            nt.at[prow(to), :], ntall.at[:, trow(d)], nt_send.at[to], nt_recv.at[d], {"dp": to}
        )

    def nt_from(s):
        return remote(nt.at[prow(d), :], ntall.at[:, trow(s)], nt_send.at[s], nt_recv.at[s], {"dp": s})

    def send_normed():
        for k in range(width // LANES):
            at = slice(k * LANES, (k + 1) * LANES)
            nt[at, :] = nrm[EDGE : EDGE + T, at].T
        for off in range(1, dp):
            go_nt(lax.rem(d + off, dp)).start()
        ntall[:, trow(d)] = nt[prow(d), :]

    def row_part(k):
        g, i = divmod(k, cuts)
        return slice(i * (R // cuts), (i + 1) * (R // cuts)), pcol(g)

    def go_rows(q, k):
        r, c = row_part(k)
        return remote(
            gout.at[q, r, c], gin.at[q, r, c], gc_send.at[q, k], gc_recv.at[q, k], {"sp": onward(q)}
        )

    def rows_step(q, k):
        r, c = row_part(k)

        @pl.when(has_in(q))
        def _():
            go_rows(q, k).wait_recv()

        @pl.when(has_out(q))
        def _():
            gout[q, r, c] = (gin[q, r, c].astype(f32) + gpl[r, c]).astype(bf16)
            go_rows(q, k).start()

    def rows_ends(g):
        @pl.when(at_end)
        def _():
            for k in range(g * cuts, (g + 1) * cuts):
                rows_step(early, k)

    def rows_early(k):
        @pl.when(jnp.logical_not(at_end))
        def _():
            rows_step(early, k)

    def rows_product(g):
        take_rest(go_dpair(g), dg_relay.at[g])
        gpl[:, pcol(g)] = mm(ntall[...], dpall[:, pcol(g)], NN)

    def rows_total(k):
        r, c = row_part(k)
        gp[r, c] = gin[0, r, c].astype(f32) + gpl[r, c] + gin[1, r, c].astype(f32)

    def pass_proj(g):
        pass_on(proj_of(g), pj_send.at[g], pj_relay.at[g])
        take_rest(proj_of(g), pj_relay.at[g])

    loads[1].wait()
    loads[2].wait()
    loads[3].wait()

    @pl.when(z > 0)
    def _():
        go_edge(0).wait_recv()

    for g in range(groups):
        before_pair(g)
    loads[4].wait()

    @pl.when(z > 0)
    def _():
        go_edge(1).wait_recv()

    pass_proj(0)
    pair_stage(0)
    chain_ends(0)
    local_mix(0)
    send_normed()
    done_early = 0
    for g in range(1, groups):
        pass_on(proj_of(g), pj_send.at[g], pj_relay.at[g])
        for _ in range(chunks // 4):
            chain_early(done_early)
            done_early += 1
        take_rest(proj_of(g), pj_relay.at[g])
        pair_stage(g)
        chain_ends(g)

    order = [(i, 0, i) for i in range(done_early, groups * chunks)]
    order += [(i + chunks // 2 + 0.5, 1, i) for i in range(groups * chunks)]
    for _, kind, i in sorted(order):
        if kind == 0:
            chain_early(i)
            continue
        chain_step(late, i)
        if (i + 1) % chunks == 0:
            g = i // chunks
            pair_grads(g)
            pair_back(g)
            if g + 1 < groups:
                local_mix(g + 1)

    for s in range(1, dp):
        nt_from(lax.rem(d + s, dp)).wait_recv()
    sent = 0
    for g in range(groups):
        pass_on(go_dpair(g), dg_send.at[g], dg_relay.at[g])
        while sent < g * cuts:
            rows_early(sent)
            sent += 1
        rows_product(g)
        rows_ends(g)
        value_grads(g)
    for k in range(width // 512):
        at = slice(k * 512, (k + 1) * 512)
        gn[:, at] = mm(dpair[...], proj[at, :], NT).astype(bf16)
    while sent < groups * cuts:
        rows_early(sent)
        sent += 1
    for g in range(groups):
        value_back(g)
    step_grads()
    for k in range(groups * cuts):
        rows_step(late, k)
        rows_total(k)

    for g in range(groups):
        drain(proj_of(g), pj_send.at[g], pj_relay.at[g])
        drain(go_dpair(g), dg_send.at[g], dg_relay.at[g])
    for off in range(1, dp):
        go_nt(lax.rem(d + off, dp)).wait_send()

    @pl.when(z < sp - 1)
    def _():
        go_edge(0).wait_send()
        go_edge(1).wait_send()

    @pl.when(z > 0)
    def _():
        for g in range(groups):
            go_next(0, g).wait_send()
            go_next(1, g).wait_send()

    for q in range(2):
        @pl.when(has_out(q))
        def _():
            for i in range(groups * chunks):
                go_state(q, i).wait_send()
            for k in range(groups * cuts):
                go_rows(q, k).wait_send()


def place_kernel(*refs):
    sources, targets, sem = refs[0:5], refs[5:10], refs[10]
    copies = [pltpu.make_async_copy(sources[k], targets[k], sem.at[k]) for k in range(5)]
    for copy in copies:
        copy.start()
    for copy in copies:
        copy.wait()


def per_device(
    normed,
    values,
    gate_in,
    step_raw,
    upstream,
    proj_pair,
    conv_value,
    conv_pair,
    step_bias,
    decay_log,
    skip,
):
    sp = lax.axis_size("sp")
    dp = lax.axis_size("dp")
    T = normed.shape[1]
    width = normed.shape[2]
    W = values.shape[2]
    heads = step_raw.shape[2]
    cols = proj_pair.shape[1]
    groups = cols // PAIR
    R = proj_pair.shape[0]
    chunks = min(8, W // groups // LANES)
    cuts = 4
    vmem = pl.BlockSpec(memory_space=pltpu.VMEM)
    hbm = pl.BlockSpec(memory_space=pltpu.HBM)
    V = pltpu.VMEM
    dma = pltpu.SemaphoreType.DMA
    vt = W // LANES
    pt = cols // LANES
    scratch = [
        V((heads, T), bf16),
        V((4, W), f32),
        V((4, cols), f32),
        V((1, heads), f32),
        V((1, heads), f32),
        V((1, heads), f32),
        V((EDGE + T, width), bf16),
        V((EDGE + T, W), bf16),
        V((T, W), bf16),
        V((T, W), bf16),
        V((width, cols), bf16),
        V((width, T), bf16),
        V((R, dp * T), bf16),
        V((T, W), bf16),
        V((vt, EDGE + T, LANES), f32),
        V((T, W), f32),
        V((T, W), f32),
        V((T, W), f32),
        V((T, W), bf16),
        V((T, W), bf16),
        V((T, W), bf16),
        V((heads, T, T), f32),
        V((groups, T, T), bf16),
        V((groups, T, T), f32),
        V((pt, EDGE + T, LANES), f32),
        V((pt, T, LANES), bf16),
        V((pt, T, LANES), f32),
        V((1, W), f32),
        V((2, STATE, W), f32),
        V((2, STATE, W), bf16),
        V((2, STATE, W), bf16),
        V((T, W), f32),
        V((T, W), f32),
        V((2, T + NEXT, W), f32),
        V((vt, T + NEXT, LANES), f32),
        V((pt, T + NEXT, LANES), f32),
        V((T, cols), bf16),
        V((dp * T, cols), bf16),
        V((R, cols), f32),
        V((2, R, cols), bf16),
        V((2, R, cols), bf16),
        dma((11,)),
        dma((2, 2)),
        dma((groups, dp)),
        dma((groups, dp)),
        dma((groups, dp)),
        dma((2, groups * chunks)),
        dma((2, groups * chunks)),
        dma((2, 2, groups)),
        dma((dp,)),
        dma((dp,)),
        dma((groups, dp)),
        dma((groups, dp)),
        dma((groups, dp)),
        dma((2, groups * cuts)),
        dma((2, groups * cuts)),
    ]
    gn, gv, gg, gs, gp = pl.pallas_call(
        functools.partial(mixer_kernel, sp, dp, heads, groups, chunks, cuts),
        out_shape=(
            jax.ShapeDtypeStruct((T, width), bf16),
            jax.ShapeDtypeStruct((T, W), bf16),
            jax.ShapeDtypeStruct((T, W), bf16),
            jax.ShapeDtypeStruct((heads, T), bf16),
            jax.ShapeDtypeStruct((R, cols), f32),
        ),
        in_specs=[hbm] * 11,
        out_specs=(vmem,) * 5,
        scratch_shapes=scratch,
        compiler_params=pltpu.CompilerParams(
            collective_id=0, has_side_effects=True, vmem_limit_bytes=40 * 1024 * 1024
        ),
    )(
        *[
            pltpu.with_memory_space_constraint(x, pltpu.HBM)
            for x in (
                normed[0],
                values[0],
                gate_in[0],
                upstream[0],
                proj_pair,
                step_raw[0].T,
                conv_value,
                conv_pair,
                step_bias[None],
                decay_log[None],
                skip[None],
            )
        ]
    )
    results = (gn, gv, gg, gs, gp)
    gn, gv, gg, gs, gp = pl.pallas_call(
        place_kernel,
        out_shape=tuple(jax.ShapeDtypeStruct(r.shape, r.dtype) for r in results),
        in_specs=[vmem] * 5,
        out_specs=(hbm,) * 5,
        scratch_shapes=[dma((5,))],
        compiler_params=pltpu.CompilerParams(vmem_limit_bytes=8 * 1024 * 1024),
    )(*results)
    return (gn[None], gv[None], gg[None], gs.T[None], gp)


def solution(mesh):
    tok = P("dp", "sp", None)
    in_specs = (tok, tok, tok, tok, tok, P("dp", None), P(), P(), P(), P(), P())
    out_specs = (tok, tok, tok, tok, P("dp", None))
    return jax.shard_map(
        per_device, mesh=mesh, in_specs=in_specs, out_specs=out_specs, check_vma=False
    )
```

```python
import functools

import jax
import jax.numpy as jnp
from jax import lax
from jax.experimental import pallas as pl
from jax.experimental.pallas import tpu as pltpu
from jax.sharding import PartitionSpec as P

HEAD = 64
STATE = 128
LANES = 128
PAIR = 2 * STATE
EDGE = 16
NEXT = 8
exact = lax.Precision.HIGHEST
f32 = jnp.float32
bf16 = jnp.bfloat16

NN = (((1,), (0,)), ((), ()))
NT = (((1,), (1,)), ((), ()))
TN = (((0,), (0,)), ((), ()))


def mm(a, b, dims):
    return lax.dot_general(a, b, dims, preferred_element_type=f32)


def mm_exact(a, b, dims):
    return lax.dot_general(a, b, dims, precision=exact, preferred_element_type=f32)


def mm_split(a, b, dims):
    high = a.astype(bf16)
    low = (a - high.astype(f32)).astype(bf16)
    return mm(high, b, dims) + mm(low, b, dims)


def silu_parts(s):
    sig = jax.nn.sigmoid(s)
    return s * sig, sig * (1.0 + s * (1.0 - sig))


def mixer_kernel(
    sp,
    dp,
    heads,
    groups,
    chunks,
    cuts,
    normed_in,
    values_in,
    gate_in,
    up_in,
    proj_in,
    step_in,
    tap_v_in,
    tap_p_in,
    bias_in,
    log_rate_in,
    skip_in,
    gn,
    gv,
    gg,
    gs,
    gp,
    step,
    tap_v,
    tap_p,
    bias,
    log_rate,
    skip,
    nrm,
    val,
    gate,
    up,
    proj,
    nt,
    ntall,
    cot,
    xvb,
    us,
    slv,
    upslope,
    xb,
    xeb,
    edy,
    dec,
    dgs,
    gm,
    pairx,
    bc,
    slp,
    ee,
    car,
    cin,
    cout,
    ybuf,
    dxl,
    zbuf,
    dvb,
    dpb,
    dpn,
    dpair,
    dpall,
    gpl,
    gin,
    gout,
    loc_sem,
    edge_sem,
    pj_send,
    pj_recv,
    pj_relay,
    ch_send,
    ch_recv,
    nx_sem,
    nt_send,
    nt_recv,
    dg_send,
    dg_recv,
    dg_relay,
    gc_send,
    gc_recv,
):
    z = lax.axis_index("sp")
    d = lax.axis_index("dp")
    T = cot.shape[0]
    W = cot.shape[1]
    width = nt.shape[0]
    R = proj_in.shape[0]
    GW = W // groups
    tiles = GW // LANES
    CW = GW // chunks
    nch = dp // 2
    core = lax.rem(d, 2)
    chip = d // 2
    sib = d + 1 - 2 * core
    first = z == 0
    last = z == sp - 1

    def remote(src, dst, ss, rs, to):
        return pltpu.make_async_remote_copy(
            src_ref=src,
            dst_ref=dst,
            send_sem=ss,
            recv_sem=rs,
            device_id=to,
            device_id_type=pl.DeviceIdType.MESH,
        )

    def prow(s):
        return pl.ds(pl.multiple_of(s * R, 16), R)

    def twice(s):
        return pl.ds(pl.multiple_of(s * 2 * T, LANES), 2 * T)

    def sent_rows(s):
        return pl.ds(pl.multiple_of(s * 2 * T + T - EDGE, EDGE), EDGE + T)

    def pcol(g):
        return slice(g * PAIR, (g + 1) * PAIR)

    below = lax.max(z - 1, 0)
    above = lax.min(z + 1, sp - 1)

    loads = [
        pltpu.make_async_copy(proj_in, proj.at[prow(d), :], loc_sem.at[0]),
        pltpu.make_async_copy(gate_in, gate, loc_sem.at[1]),
        pltpu.make_async_copy(up_in, up, loc_sem.at[2]),
        pltpu.make_async_copy(values_in, val.at[EDGE : EDGE + T, :], loc_sem.at[3]),
        pltpu.make_async_copy(normed_in, nrm.at[EDGE : EDGE + T, :], loc_sem.at[4]),
    ]
    small = [
        pltpu.make_async_copy(src, dst, loc_sem.at[5 + k])
        for k, (src, dst) in enumerate(
            (
                (step_in, step),
                (bias_in, bias),
                (log_rate_in, log_rate),
                (skip_in, skip),
                (tap_v_in, tap_v),
                (tap_p_in, tap_p),
            )
        )
    ]
    loads[0].start()
    for load in small + loads[1:]:
        load.start()

    barrier = pltpu.get_barrier_semaphore()
    for off in range(1, dp):
        pl.semaphore_signal(
            barrier,
            inc=1,
            device_id={"dp": lax.rem(d + off, dp)},
            device_id_type=pl.DeviceIdType.MESH,
        )

    @pl.when(z > 0)
    def _():
        pl.semaphore_signal(
            barrier, inc=1, device_id={"sp": below}, device_id_type=pl.DeviceIdType.MESH
        )

    @pl.when(z < sp - 1)
    def _():
        pl.semaphore_signal(
            barrier, inc=1, device_id={"sp": above}, device_id_type=pl.DeviceIdType.MESH
        )

    arrivals = dp - 1 + jnp.where(first, 0, 1) + jnp.where(last, 0, 1)
    pl.semaphore_wait(barrier, arrivals)

    def go_proj(g, s, to, ss):
        at = proj.at[prow(s), pcol(g)]
        return remote(at, at, ss, pj_recv.at[g, s], {"dp": to})

    def chip_peer(off):
        return lax.rem(chip + off, nch) * 2 + core

    def spread_out(go, send):
        for off in range(1, nch):
            to = chip_peer(off)
            go(d, to, send.at[to]).start()
        go(d, sib, send.at[sib]).start()

    def pass_on(go, send, relay):
        for off in range(1, nch):
            s = chip_peer(off)
            go(s, sib, relay.at[s]).wait_recv()
            go(s, sib, relay.at[s]).start()

    def take_rest(go, relay):
        go(sib, sib, relay.at[sib]).wait_recv()
        for off in range(1, nch):
            s = chip_peer(off) + 1 - 2 * core
            go(s, sib, relay.at[s]).wait_recv()

    def drain(go, send, relay):
        for off in range(1, nch):
            to = chip_peer(off)
            go(d, to, send.at[to]).wait_send()
            go(to, sib, relay.at[to]).wait_send()
        go(d, sib, send.at[sib]).wait_send()

    def proj_of(g):
        return lambda s, to, ss: go_proj(g, s, to, ss)

    loads[0].wait()
    spread_out(proj_of(0), pj_send.at[0])

    def go_edge(k):
        src = (values_in, normed_in)[k]
        dst = (val, nrm)[k]
        return remote(
            src.at[T - EDGE : T, :], dst.at[0:EDGE, :], edge_sem.at[0, k], edge_sem.at[1, k], {"sp": above}
        )

    @pl.when(z < sp - 1)
    def _():
        go_edge(0).start()
        go_edge(1).start()

    for g in range(1, groups):
        spread_out(proj_of(g), pj_send.at[g])

    pieces = dpb.shape[0]
    dpb[:, 0:EDGE, :] = jnp.zeros((pieces, EDGE, LANES), f32)
    dpb[:, EDGE + T : EDGE + T + NEXT, :] = jnp.zeros((pieces, NEXT, LANES), f32)
    for s in range(dp):
        dpall[s * 2 * T : s * 2 * T + T - EDGE, :] = jnp.zeros((T - EDGE, dpall.shape[1]), bf16)

    @pl.when(first)
    def _():
        val[0:EDGE, :] = jnp.zeros((EDGE, W), bf16)
        nrm[0:EDGE, :] = jnp.zeros((EDGE, width), bf16)
        cin[0] = jnp.zeros((STATE, W), bf16)
        gin[0] = jnp.zeros(gin.shape[1:], bf16)

    @pl.when(last)
    def _():
        cin[1] = jnp.zeros((STATE, W), bf16)
        gin[1] = jnp.zeros(gin.shape[1:], bf16)
        dvb[:, T : T + NEXT, :] = jnp.zeros((dvb.shape[0], NEXT, LANES), f32)
        dpn[...] = jnp.zeros(dpn.shape, f32)

    for load in small:
        load.wait()
    row_i = lax.broadcasted_iota(jnp.int32, (T, T), 0)
    col_i = lax.broadcasted_iota(jnp.int32, (T, T), 1)
    causal = row_i >= col_i
    tri = causal.astype(f32)
    lane = lax.broadcasted_iota(jnp.int32, (T, LANES), 1)
    low = lane < HEAD

    def padded(v):
        return jnp.concatenate([v, jnp.zeros((v.shape[0], LANES - heads), f32)], axis=1)

    def spread(x, j):
        a = x[:, 2 * j : 2 * j + 1]
        b = x[:, 2 * j + 1 : 2 * j + 2]
        mask = low if x.shape[0] == T else low[0 : x.shape[0]]
        return jnp.where(mask, a, b)

    rate = -jnp.exp(padded(log_rate[...]))
    skips = padded(skip[...])
    steps = jnp.concatenate([step[...].astype(f32), jnp.zeros((LANES - heads, T), f32)], axis=0)
    raw = steps.T + padded(bias[...])
    dt = jax.nn.softplus(raw)
    sgs = jax.nn.sigmoid(raw)
    ac = mm_exact(tri, dt * rate, NN)
    ac_t = ac.T
    ea = jnp.exp(ac)
    end = ac[T - 1 : T, :]
    te = jnp.exp(end - ac)
    e_end = jnp.exp(end)

    def halves(v):
        zero = jnp.zeros_like(v)
        return jnp.concatenate([jnp.where(low, v, zero), jnp.where(low, zero, v)], axis=0)

    def conv(buf, k, taps, at):
        total = taps[0:1, at] * buf[k, EDGE - 3 : EDGE - 3 + T, :]
        for i in range(1, 4):
            total = total + taps[i : i + 1, at] * buf[k, EDGE - 3 + i : EDGE - 3 + i + T, :]
        return total

    def conv_back(buf, k, taps, at, start=0, count=T):
        total = taps[3:4, at] * buf[k, start : start + count, :]
        for i in range(3):
            total = total + taps[i : i + 1, at] * buf[k, start + 3 - i : start + 3 - i + count, :]
        return total

    def before_pair(g):
        d_g = jnp.zeros((T, T), f32)
        for j in range(g * tiles, (g + 1) * tiles):
            at = slice(j * LANES, (j + 1) * LANES)
            v = gate[:, at].astype(f32)
            upf = up[:, at].astype(f32)
            act, slope = silu_parts(v)
            dy = (upf * act).astype(bf16)
            cot[:, at] = dy
            upslope[:, at] = upf * slope
            xvb[j] = val[:, at].astype(f32)
            u, slope = silu_parts(conv(xvb, j, tap_v, at))
            us[:, at] = u
            slv[:, at] = slope
            x = (u * spread(dt, j)).astype(bf16)
            xb[:, at] = x
            xeb[:, at] = (x.astype(f32) * spread(te, j)).astype(bf16)
            edy[:, at] = (spread(ea, j) * dy.astype(f32)).astype(bf16)
            ee[:, at] = spread(e_end, j)
            d_mix = mm(halves(dy), x, NT)
            for q in range(2):
                h = 2 * j + q
                diff = ac[:, h : h + 1] - ac_t[h : h + 1, :]
                decay = jnp.exp(jnp.where(causal, diff, -1e30))
                dec[h] = decay
                d_g = d_g + d_mix[q * T : (q + 1) * T] * decay
        dgs[g] = d_g.astype(bf16)

    def pair_stage(g):
        lanes = slice(g * GW, (g + 1) * GW)
        pb = mm(nrm[...], proj[:, pcol(g)], NN).astype(bf16).astype(f32)
        for i in range(2):
            k = 2 * g + i
            at = slice(k * LANES, (k + 1) * LANES)
            pairx[k] = pb[:, i * LANES : (i + 1) * LANES]
            act, slope = silu_parts(conv(pairx, k, tap_p, at))
            bc[k] = act.astype(bf16)
            slp[k] = slope
        b = bc[2 * g]
        cc = bc[2 * g + 1]
        gm[g] = mm(cc, b, NT)
        car[0, :, lanes] = mm(b, xeb[:, lanes], TN)
        car[1, :, lanes] = mm(cc, edy[:, lanes], TN)

    def local_mix(g):
        gmat = gm[g]
        for j in range(g * tiles, (g + 1) * tiles):
            at = slice(j * LANES, (j + 1) * LANES)
            mixes = [(gmat * dec[2 * j + q]).astype(bf16) for q in range(2)]
            ybuf[:, at] = mm(jnp.concatenate(mixes, axis=1), halves(xb[:, at]), NN)
            dxl[:, at] = mm(jnp.concatenate(mixes, axis=0), halves(cot[:, at]), TN)

    def has_in(q):
        return jnp.where(q == 0, z > 0, z < sp - 1)

    def has_out(q):
        return jnp.where(q == 0, z < sp - 1, z > 0)

    def onward(q):
        return lax.max(lax.min(z + 1 - 2 * q, sp - 1), 0)

    def go_state(q, i):
        lanes = slice(i * CW, (i + 1) * CW)
        return remote(
            cout.at[q, :, lanes], cin.at[q, :, lanes], ch_send.at[q, i], ch_recv.at[q, i], {"sp": onward(q)}
        )

    def chain_step(q, i):
        lanes = slice(i * CW, (i + 1) * CW)

        @pl.when(has_in(q))
        def _():
            go_state(q, i).wait_recv()

        @pl.when(has_out(q))
        def _():
            total = cin[q, :, lanes].astype(f32) * ee[0:1, lanes] + car[q, :, lanes]
            cout[q, :, lanes] = total.astype(bf16)
            go_state(q, i).start()

    def chain_ends(g):
        @pl.when(at_end)
        def _():
            for i in range(g * chunks, (g + 1) * chunks):
                chain_step(early, i)

    def chain_early(i):
        @pl.when(jnp.logical_not(at_end))
        def _():
            chain_step(early, i)

    early = jnp.where(z < sp // 2, 0, 1)
    late = 1 - early
    at_end = (z == 0) | (z == sp - 1)

    def go_next(kind, g):
        if kind == 0:
            part = slice(2 * g, 2 * g + 2)
            src, dst = dpb.at[part, EDGE : EDGE + NEXT, :], dpn.at[part]
        else:
            part = slice(g * tiles, (g + 1) * tiles)
            src, dst = dvb.at[part, 0:NEXT, :], dvb.at[part, T : T + NEXT, :]
        return remote(
            src,
            dst,
            nx_sem.at[0, kind, g],
            nx_sem.at[1, kind, g],
            {"sp": below},
        )

    def send_next(kind, g):
        @pl.when(z > 0)
        def _():
            go_next(kind, g).start()

    def take_next(kind, g):
        @pl.when(z < sp - 1)
        def _():
            go_next(kind, g).wait_recv()

    def pair_grads(g):
        lanes = slice(g * GW, (g + 1) * GW)
        b = bc[2 * g]
        cc = bc[2 * g + 1]
        dg = dgs[g]
        d_b = mm(dg, cc, TN) + mm(xeb[:, lanes], cin[1, :, lanes], NT)
        d_c = mm(dg, b, NN) + mm(edy[:, lanes], cin[0, :, lanes], NT)
        for k, part in ((2 * g, d_b), (2 * g + 1, d_c)):
            at = slice(k * LANES, (k + 1) * LANES)
            dpb[k, EDGE : EDGE + T, :] = part * slp[k]
            dpall[sent_rows(d), at] = conv_back(dpb, k, tap_p, at, 0, EDGE + T).astype(bf16)
            spread_out(go_dpair(k), dg_send.at[k])
        send_next(0, g)

    def go_dpair(k):
        def go(s, to, ss):
            at = dpall.at[sent_rows(s), k * LANES : (k + 1) * LANES]
            return remote(at, at, ss, dg_recv.at[k, s], {"dp": to})

        return go

    def pair_back(g):
        take_next(0, g)
        for k in range(2 * g, 2 * g + 2):
            at = slice(k * LANES, (k + 1) * LANES)
            dpb[k, EDGE + T : EDGE + T + NEXT, :] = dpn[k]
            dpair[:, at] = conv_back(dpb, k, tap_p, at, EDGE).astype(bf16)

    def value_grads(g):
        b = bc[2 * g]
        cc = bc[2 * g + 1]
        for j in range(g * tiles, (g + 1) * tiles):
            at = slice(j * LANES, (j + 1) * LANES)
            s_in = cin[0, :, at]
            ds = cin[1, :, at]
            dyf = cot[:, at].astype(f32)
            u = us[:, at]
            y = ybuf[:, at] + spread(ea, j) * mm(cc, s_in, NN)
            zbuf[0, 0:T, at] = dyf * y
            ybf = (y + spread(skips, j) * u).astype(bf16)
            gg[:, at] = (upslope[:, at] * ybf.astype(f32)).astype(bf16)
            x = xb[:, at].astype(f32)
            tej = spread(te, j)
            far = mm(b, ds, NN)
            dx = dxl[:, at] + tej * far
            zbuf[1, 0:T, at] = x * dx
            ends = jnp.sum(x * tej * far, axis=0, keepdims=True) + ee[:, at] * jnp.sum(
                ds.astype(f32) * s_in.astype(f32), axis=0, keepdims=True
            )
            zbuf[1, T : T + NEXT, at] = jnp.broadcast_to(ends, (NEXT, LANES))
            du = spread(dt, j) * dx + spread(skips, j) * dyf
            dvb[j, 0:T, :] = du * slv[:, at]
        send_next(1, g)

    def value_back(g):
        take_next(1, g)
        for j in range(g * tiles, (g + 1) * tiles):
            at = slice(j * LANES, (j + 1) * LANES)
            gv[:, at] = conv_back(dvb, j, tap_v, at).astype(bf16)

    def step_grads():
        sel_r = lax.broadcasted_iota(jnp.int32, (LANES, W), 0)
        sel_c = lax.broadcasted_iota(jnp.int32, (LANES, W), 1)
        sel = jnp.where(sel_c // HEAD == sel_r, 1.0, 0.0).astype(bf16)
        r1 = mm_split(zbuf[0, 0:T, :], sel, NT)
        both = mm_split(zbuf[1], sel, NT)
        xd = both[0:T]
        d_end = both[T : T + 1]
        back = mm_exact(tri, r1 - xd, TN) + d_end
        d_dt = (xd / dt + rate * back) * sgs
        gs[...] = d_dt.T[0:heads, :].astype(bf16)

    def go_nt(to):
        return remote(
            nt.at[prow(to), :], ntall.at[:, twice(d)], nt_send.at[to], nt_recv.at[d], {"dp": to}
        )

    def nt_from(s):
        return remote(nt.at[prow(d), :], ntall.at[:, twice(s)], nt_send.at[s], nt_recv.at[s], {"dp": s})

    def send_normed():
        for k in range(width // LANES):
            at = slice(k * LANES, (k + 1) * LANES)
            nt[at, T : 2 * T] = nrm[EDGE : EDGE + T, at].T
            edge = jnp.concatenate([jnp.zeros((T - EDGE, LANES), bf16), nrm[0:EDGE, at]], axis=0)
            nt[at, 0:T] = edge.T
        for off in range(1, dp):
            go_nt(lax.rem(d + off, dp)).start()
        ntall[:, twice(d)] = nt[prow(d), :]

    def row_part(k):
        p, i = divmod(k, cuts)
        return slice(i * (R // cuts), (i + 1) * (R // cuts)), slice(p * LANES, (p + 1) * LANES)

    def go_rows(q, k):
        r, c = row_part(k)
        return remote(
            gout.at[q, r, c], gin.at[q, r, c], gc_send.at[q, k], gc_recv.at[q, k], {"sp": onward(q)}
        )

    def rows_step(q, k):
        r, c = row_part(k)

        @pl.when(has_in(q))
        def _():
            go_rows(q, k).wait_recv()

        @pl.when(has_out(q))
        def _():
            gout[q, r, c] = (gin[q, r, c].astype(f32) + gpl[r, c]).astype(bf16)
            go_rows(q, k).start()

    def rows_ends(p):
        @pl.when(at_end)
        def _():
            for k in range(p * cuts, (p + 1) * cuts):
                rows_step(early, k)

    def rows_early(k):
        @pl.when(jnp.logical_not(at_end))
        def _():
            rows_step(early, k)

    def rows_product(p):
        pass_on(go_dpair(p), dg_send.at[p], dg_relay.at[p])
        take_rest(go_dpair(p), dg_relay.at[p])
        at = slice(p * LANES, (p + 1) * LANES)
        gpl[:, at] = mm(ntall[...], dpall[:, at], NN)
        rows_ends(p)

    def rows_total(k):
        r, c = row_part(k)
        gp[r, c] = gin[0, r, c].astype(f32) + gpl[r, c] + gin[1, r, c].astype(f32)

    def pass_proj(g):
        pass_on(proj_of(g), pj_send.at[g], pj_relay.at[g])
        take_rest(proj_of(g), pj_relay.at[g])

    loads[1].wait()
    loads[2].wait()
    loads[3].wait()

    @pl.when(z > 0)
    def _():
        go_edge(0).wait_recv()

    for g in range(groups):
        before_pair(g)
    loads[4].wait()

    @pl.when(z > 0)
    def _():
        go_edge(1).wait_recv()

    pass_proj(0)
    pair_stage(0)
    chain_ends(0)
    local_mix(0)
    send_normed()
    done_early = 0
    for g in range(1, groups):
        pass_on(proj_of(g), pj_send.at[g], pj_relay.at[g])
        for _ in range(chunks // 4):
            chain_early(done_early)
            done_early += 1
        take_rest(proj_of(g), pj_relay.at[g])
        pair_stage(g)
        chain_ends(g)

    order = [(i, 0, i) for i in range(done_early, groups * chunks)]
    order += [(i + chunks // 2 + 0.5, 1, i) for i in range(groups * chunks)]
    for _, kind, i in sorted(order):
        if kind == 0:
            chain_early(i)
            continue
        chain_step(late, i)
        if (i + 1) % chunks == 0:
            g = i // chunks
            pair_grads(g)
            if g + 1 < groups:
                local_mix(g + 1)

    for s in range(1, dp):
        nt_from(lax.rem(d + s, dp)).wait_recv()
    for g in range(groups):
        rows_product(2 * g)
        rows_product(2 * g + 1)
        if g + 1 < groups:
            value_grads(g)
    tail = groups - 1
    for k in range(2 * tail * cuts):
        rows_early(k)
    value_grads(tail)
    for g in range(groups):
        pair_back(g)
    for k in range(width // 512):
        at = slice(k * 512, (k + 1) * 512)
        gn[:, at] = mm(dpair[...], proj[at, :], NT).astype(bf16)
    for k in range(2 * tail * cuts, pieces * cuts):
        rows_early(k)
    for k in range(2 * tail * cuts):
        rows_step(late, k)
        rows_total(k)
    for g in range(groups):
        value_back(g)
    step_grads()
    for k in range(2 * tail * cuts, pieces * cuts):
        rows_step(late, k)
        rows_total(k)

    for g in range(groups):
        drain(proj_of(g), pj_send.at[g], pj_relay.at[g])
    for k in range(pieces):
        drain(go_dpair(k), dg_send.at[k], dg_relay.at[k])
    for off in range(1, dp):
        go_nt(lax.rem(d + off, dp)).wait_send()

    @pl.when(z < sp - 1)
    def _():
        go_edge(0).wait_send()
        go_edge(1).wait_send()

    @pl.when(z > 0)
    def _():
        for g in range(groups):
            go_next(0, g).wait_send()
            go_next(1, g).wait_send()

    for q in range(2):
        @pl.when(has_out(q))
        def _():
            for i in range(groups * chunks):
                go_state(q, i).wait_send()
            for k in range(pieces * cuts):
                go_rows(q, k).wait_send()


def place_kernel(*refs):
    sources, targets, sem = refs[0:5], refs[5:10], refs[10]
    copies = [pltpu.make_async_copy(sources[k], targets[k], sem.at[k]) for k in range(5)]
    for copy in copies:
        copy.start()
    for copy in copies:
        copy.wait()


def per_device(
    normed,
    values,
    gate_in,
    step_raw,
    upstream,
    proj_pair,
    conv_value,
    conv_pair,
    step_bias,
    decay_log,
    skip,
):
    sp = lax.axis_size("sp")
    dp = lax.axis_size("dp")
    T = normed.shape[1]
    width = normed.shape[2]
    W = values.shape[2]
    heads = step_raw.shape[2]
    cols = proj_pair.shape[1]
    groups = cols // PAIR
    R = proj_pair.shape[0]
    chunks = min(8, W // groups // LANES)
    cuts = 4
    vmem = pl.BlockSpec(memory_space=pltpu.VMEM)
    hbm = pl.BlockSpec(memory_space=pltpu.HBM)
    V = pltpu.VMEM
    dma = pltpu.SemaphoreType.DMA
    vt = W // LANES
    pt = cols // LANES
    scratch = [
        V((heads, T), bf16),
        V((4, W), f32),
        V((4, cols), f32),
        V((1, heads), f32),
        V((1, heads), f32),
        V((1, heads), f32),
        V((EDGE + T, width), bf16),
        V((EDGE + T, W), bf16),
        V((T, W), bf16),
        V((T, W), bf16),
        V((width, cols), bf16),
        V((width, 2 * T), bf16),
        V((R, dp * 2 * T), bf16),
        V((T, W), bf16),
        V((vt, EDGE + T, LANES), f32),
        V((T, W), f32),
        V((T, W), f32),
        V((T, W), f32),
        V((T, W), bf16),
        V((T, W), bf16),
        V((T, W), bf16),
        V((heads, T, T), f32),
        V((groups, T, T), bf16),
        V((groups, T, T), f32),
        V((pt, EDGE + T, LANES), f32),
        V((pt, T, LANES), bf16),
        V((pt, T, LANES), f32),
        V((1, W), f32),
        V((2, STATE, W), f32),
        V((2, STATE, W), bf16),
        V((2, STATE, W), bf16),
        V((T, W), f32),
        V((T, W), f32),
        V((2, T + NEXT, W), f32),
        V((vt, T + NEXT, LANES), f32),
        V((pt, EDGE + T + NEXT, LANES), f32),
        V((pt, NEXT, LANES), f32),
        V((T, cols), bf16),
        V((dp * 2 * T, cols), bf16),
        V((R, cols), f32),
        V((2, R, cols), bf16),
        V((2, R, cols), bf16),
        dma((11,)),
        dma((2, 2)),
        dma((groups, dp)),
        dma((groups, dp)),
        dma((groups, dp)),
        dma((2, groups * chunks)),
        dma((2, groups * chunks)),
        dma((2, 2, groups)),
        dma((dp,)),
        dma((dp,)),
        dma((pt, dp)),
        dma((pt, dp)),
        dma((pt, dp)),
        dma((2, pt * cuts)),
        dma((2, pt * cuts)),
    ]
    gn, gv, gg, gs, gp = pl.pallas_call(
        functools.partial(mixer_kernel, sp, dp, heads, groups, chunks, cuts),
        out_shape=(
            jax.ShapeDtypeStruct((T, width), bf16),
            jax.ShapeDtypeStruct((T, W), bf16),
            jax.ShapeDtypeStruct((T, W), bf16),
            jax.ShapeDtypeStruct((heads, T), bf16),
            jax.ShapeDtypeStruct((R, cols), f32),
        ),
        in_specs=[hbm] * 11,
        out_specs=(vmem,) * 5,
        scratch_shapes=scratch,
        compiler_params=pltpu.CompilerParams(
            collective_id=0, has_side_effects=True, vmem_limit_bytes=40 * 1024 * 1024
        ),
    )(
        *[
            pltpu.with_memory_space_constraint(x, pltpu.HBM)
            for x in (
                normed[0],
                values[0],
                gate_in[0],
                upstream[0],
                proj_pair,
                step_raw[0].T,
                conv_value,
                conv_pair,
                step_bias[None],
                decay_log[None],
                skip[None],
            )
        ]
    )
    results = (gn, gv, gg, gs, gp)
    gn, gv, gg, gs, gp = pl.pallas_call(
        place_kernel,
        out_shape=tuple(jax.ShapeDtypeStruct(r.shape, r.dtype) for r in results),
        in_specs=[vmem] * 5,
        out_specs=(hbm,) * 5,
        scratch_shapes=[dma((5,))],
        compiler_params=pltpu.CompilerParams(vmem_limit_bytes=8 * 1024 * 1024),
    )(*results)
    return (gn[None], gv[None], gg[None], gs.T[None], gp)


def solution(mesh):
    tok = P("dp", "sp", None)
    in_specs = (tok, tok, tok, tok, tok, P("dp", None), P(), P(), P(), P(), P())
    out_specs = (tok, tok, tok, tok, P("dp", None))
    return jax.shard_map(
        per_device, mesh=mesh, in_specs=in_specs, out_specs=out_specs, check_vma=False
    )
```

```python
import functools

import jax
import jax.numpy as jnp
from jax import lax
from jax.experimental import pallas as pl
from jax.experimental.pallas import tpu as pltpu
from jax.sharding import PartitionSpec as P

HEAD = 64
STATE = 128
LANES = 128
PAIR = 2 * STATE
EDGE = 16
NEXT = 8
exact = lax.Precision.HIGHEST
f32 = jnp.float32
bf16 = jnp.bfloat16

NN = (((1,), (0,)), ((), ()))
NT = (((1,), (1,)), ((), ()))
TN = (((0,), (0,)), ((), ()))


def mm(a, b, dims):
    return lax.dot_general(a, b, dims, preferred_element_type=f32)


def mm_exact(a, b, dims):
    return lax.dot_general(a, b, dims, precision=exact, preferred_element_type=f32)


def mm_split(a, b, dims):
    high = a.astype(bf16)
    low = (a - high.astype(f32)).astype(bf16)
    return mm(high, b, dims) + mm(low, b, dims)


def silu_parts(s):
    sig = jax.nn.sigmoid(s)
    return s * sig, sig * (1.0 + s * (1.0 - sig))


def mixer_kernel(
    sp,
    dp,
    heads,
    groups,
    chunks,
    cuts,
    normed_in,
    values_in,
    gate_in,
    up_in,
    proj_in,
    step_in,
    tap_v_in,
    tap_p_in,
    bias_in,
    log_rate_in,
    skip_in,
    gn,
    gv,
    gg,
    gs,
    gp,
    step,
    tap_v,
    tap_p,
    bias,
    log_rate,
    skip,
    nrm,
    val,
    gate,
    up,
    proj,
    nt,
    ntall,
    cot,
    xvb,
    us,
    slv,
    upslope,
    xb,
    tx,
    dec,
    dgs,
    gm,
    pairx,
    bc,
    bct,
    slp,
    ee,
    car,
    cin,
    cout,
    ybuf,
    dxl,
    zbuf,
    dvb,
    dpb,
    dpn,
    dpair,
    dpall,
    gpl,
    gin,
    gout,
    loc_sem,
    edge_sem,
    pj_send,
    pj_recv,
    pj_relay,
    ch_send,
    ch_recv,
    nx_sem,
    nt_send,
    nt_recv,
    dg_send,
    dg_recv,
    dg_relay,
    gc_send,
    gc_recv,
):
    z = lax.axis_index("sp")
    d = lax.axis_index("dp")
    T = cot.shape[0]
    W = cot.shape[1]
    width = nt.shape[0]
    R = proj_in.shape[0]
    GW = W // groups
    tiles = GW // LANES
    CW = GW // chunks
    nch = dp // 2
    core = lax.rem(d, 2)
    chip = d // 2
    sib = d + 1 - 2 * core
    first = z == 0
    last = z == sp - 1

    def remote(src, dst, ss, rs, to):
        return pltpu.make_async_remote_copy(
            src_ref=src,
            dst_ref=dst,
            send_sem=ss,
            recv_sem=rs,
            device_id=to,
            device_id_type=pl.DeviceIdType.MESH,
        )

    def prow(s):
        return pl.ds(pl.multiple_of(s * R, 16), R)

    def twice(s):
        return pl.ds(pl.multiple_of(s * 2 * T, LANES), 2 * T)

    def sent_rows(s):
        return pl.ds(pl.multiple_of(s * 2 * T + T - EDGE, EDGE), EDGE + T)

    def pcol(g):
        return slice(g * PAIR, (g + 1) * PAIR)

    below = lax.max(z - 1, 0)
    above = lax.min(z + 1, sp - 1)

    loads = [
        pltpu.make_async_copy(proj_in, proj.at[prow(d), :], loc_sem.at[0]),
        pltpu.make_async_copy(gate_in, gate, loc_sem.at[1]),
        pltpu.make_async_copy(up_in, up, loc_sem.at[2]),
        pltpu.make_async_copy(values_in, val.at[EDGE : EDGE + T, :], loc_sem.at[3]),
        pltpu.make_async_copy(normed_in, nrm.at[EDGE : EDGE + T, :], loc_sem.at[4]),
    ]
    small = [
        pltpu.make_async_copy(src, dst, loc_sem.at[5 + k])
        for k, (src, dst) in enumerate(
            (
                (step_in, step),
                (bias_in, bias),
                (log_rate_in, log_rate),
                (skip_in, skip),
                (tap_v_in, tap_v),
                (tap_p_in, tap_p),
            )
        )
    ]
    loads[0].start()
    for load in small + loads[1:]:
        load.start()

    barrier = pltpu.get_barrier_semaphore()
    for off in range(1, dp):
        pl.semaphore_signal(
            barrier,
            inc=1,
            device_id={"dp": lax.rem(d + off, dp)},
            device_id_type=pl.DeviceIdType.MESH,
        )

    @pl.when(z > 0)
    def _():
        pl.semaphore_signal(
            barrier, inc=1, device_id={"sp": below}, device_id_type=pl.DeviceIdType.MESH
        )

    @pl.when(z < sp - 1)
    def _():
        pl.semaphore_signal(
            barrier, inc=1, device_id={"sp": above}, device_id_type=pl.DeviceIdType.MESH
        )

    arrivals = dp - 1 + jnp.where(first, 0, 1) + jnp.where(last, 0, 1)
    pl.semaphore_wait(barrier, arrivals)

    def go_proj(g, s, to, ss):
        at = proj.at[prow(s), pcol(g)]
        return remote(at, at, ss, pj_recv.at[g, s], {"dp": to})

    def chip_peer(off):
        if nch & (nch - 1):
            return lax.rem(chip + off, nch) * 2 + core
        to = chip
        for bit in range(off.bit_length()):
            if off >> bit & 1:
                to = to + (1 - 2 * lax.rem(chip // 2**bit, 2)) * 2**bit
        return to * 2 + core

    far_first = sorted(range(1, nch), key=lambda off: (-bin(off).count("1"), off))

    def spread_out(go, send):
        for off in far_first:
            to = chip_peer(off)
            go(d, to, send.at[to]).start()
        go(d, sib, send.at[sib]).start()

    def pass_on(go, send, relay):
        for off in far_first:
            s = chip_peer(off)
            go(s, sib, relay.at[s]).wait_recv()
            go(s, sib, relay.at[s]).start()

    def take_rest(go, relay):
        go(sib, sib, relay.at[sib]).wait_recv()
        for off in range(1, nch):
            s = chip_peer(off) + 1 - 2 * core
            go(s, sib, relay.at[s]).wait_recv()

    def drain(go, send, relay):
        for off in range(1, nch):
            to = chip_peer(off)
            go(d, to, send.at[to]).wait_send()
            go(to, sib, relay.at[to]).wait_send()
        go(d, sib, send.at[sib]).wait_send()

    def proj_of(g):
        return lambda s, to, ss: go_proj(g, s, to, ss)

    loads[0].wait()
    spread_out(proj_of(0), pj_send.at[0])

    def go_edge(k):
        src = (values_in, normed_in)[k]
        dst = (val, nrm)[k]
        return remote(
            src.at[T - EDGE : T, :], dst.at[0:EDGE, :], edge_sem.at[0, k], edge_sem.at[1, k], {"sp": above}
        )

    @pl.when(z < sp - 1)
    def _():
        go_edge(0).start()
        go_edge(1).start()

    for g in range(1, groups):
        spread_out(proj_of(g), pj_send.at[g])

    pieces = dpb.shape[0]
    dpb[:, 0:EDGE, :] = jnp.zeros((pieces, EDGE, LANES), f32)
    dpb[:, EDGE + T : EDGE + T + NEXT, :] = jnp.zeros((pieces, NEXT, LANES), f32)
    for s in range(dp):
        dpall[s * 2 * T : s * 2 * T + T - EDGE, :] = jnp.zeros((T - EDGE, dpall.shape[1]), bf16)

    @pl.when(first)
    def _():
        val[0:EDGE, :] = jnp.zeros((EDGE, W), bf16)
        nrm[0:EDGE, :] = jnp.zeros((EDGE, width), bf16)
        cin[0] = jnp.zeros((STATE, W), bf16)
        gin[0] = jnp.zeros(gin.shape[1:], bf16)

    @pl.when(last)
    def _():
        cin[1] = jnp.zeros((STATE, W), bf16)
        gin[1] = jnp.zeros(gin.shape[1:], bf16)
        dvb[:, T : T + NEXT, :] = jnp.zeros((dvb.shape[0], NEXT, LANES), f32)
        dpn[...] = jnp.zeros(dpn.shape, f32)

    for load in small:
        load.wait()
    row_i = lax.broadcasted_iota(jnp.int32, (T, T), 0)
    col_i = lax.broadcasted_iota(jnp.int32, (T, T), 1)
    causal = row_i >= col_i
    tri = causal.astype(f32)
    lane = lax.broadcasted_iota(jnp.int32, (T, LANES), 1)
    low = lane < HEAD

    def padded(v):
        return jnp.concatenate([v, jnp.zeros((v.shape[0], LANES - heads), f32)], axis=1)

    def spread(x, j):
        a = x[:, 2 * j : 2 * j + 1]
        b = x[:, 2 * j + 1 : 2 * j + 2]
        mask = low if x.shape[0] == T else low[0 : x.shape[0]]
        return jnp.where(mask, a, b)

    rate = -jnp.exp(padded(log_rate[...]))
    skips = padded(skip[...])
    steps = jnp.concatenate([step[...].astype(f32), jnp.zeros((LANES - heads, T), f32)], axis=0)
    raw = steps.T + padded(bias[...])
    dt = jax.nn.softplus(raw)
    sgs = jax.nn.sigmoid(raw)
    ac = mm_exact(tri, dt * rate, NN)
    ac_t = ac.T
    ea = jnp.exp(ac)
    end = ac[T - 1 : T, :]
    te = jnp.exp(end - ac)
    e_end = jnp.exp(end)

    def halves(v):
        zero = jnp.zeros_like(v)
        return jnp.concatenate([jnp.where(low, v, zero), jnp.where(low, zero, v)], axis=0)

    def conv(buf, k, taps, at):
        total = taps[0:1, at] * buf[k, EDGE - 3 : EDGE - 3 + T, :]
        for i in range(1, 4):
            total = total + taps[i : i + 1, at] * buf[k, EDGE - 3 + i : EDGE - 3 + i + T, :]
        return total

    def conv_back(buf, k, taps, at, start=0, count=T):
        total = taps[3:4, at] * buf[k, start : start + count, :]
        for i in range(3):
            total = total + taps[i : i + 1, at] * buf[k, start + 3 - i : start + 3 - i + count, :]
        return total

    def before_pair(g):
        d_g = jnp.zeros((T, T), f32)
        for j in range(g * tiles, (g + 1) * tiles):
            at = slice(j * LANES, (j + 1) * LANES)
            v = gate[:, at].astype(f32)
            upf = up[:, at].astype(f32)
            act, slope = silu_parts(v)
            dy = (upf * act).astype(bf16)
            cot[:, at] = dy
            upslope[:, at] = upf * slope
            xvb[j] = val[:, at].astype(f32)
            u, slope = silu_parts(conv(xvb, j, tap_v, at))
            us[:, at] = u
            slv[:, at] = slope
            x = (u * spread(dt, j)).astype(bf16)
            xb[:, at] = x
            tx[0, :, at] = (x.astype(f32) * spread(te, j)).astype(bf16)
            tx[1, :, at] = (spread(ea, j) * dy.astype(f32)).astype(bf16)
            ee[:, at] = spread(e_end, j)
            d_mix = mm(halves(dy), x, NT)
            for q in range(2):
                h = 2 * j + q
                diff = ac[:, h : h + 1] - ac_t[h : h + 1, :]
                decay = jnp.exp(jnp.where(causal, diff, -1e30))
                dec[h] = decay
                d_g = d_g + d_mix[q * T : (q + 1) * T] * decay
        dgs[g, 0] = d_g.astype(bf16)
        dgs[g, 1] = d_g.T.astype(bf16)

    def has_in(q):
        return jnp.where(q == 0, z > 0, z < sp - 1)

    def has_out(q):
        return jnp.where(q == 0, z < sp - 1, z > 0)

    def onward(q):
        return lax.max(lax.min(z + 1 - 2 * q, sp - 1), 0)

    def go_state(q, i):
        lanes = slice(i * CW, (i + 1) * CW)
        return remote(
            cout.at[q, :, lanes], cin.at[q, :, lanes], ch_send.at[q, i], ch_recv.at[q, i], {"sp": onward(q)}
        )

    def chain_step(q, i):
        lanes = slice(i * CW, (i + 1) * CW)

        @pl.when(has_in(q))
        def _():
            go_state(q, i).wait_recv()

        @pl.when(has_out(q))
        def _():
            total = cin[q, :, lanes].astype(f32) * ee[0:1, lanes] + car[q, :, lanes]
            cout[q, :, lanes] = total.astype(bf16)
            go_state(q, i).start()

    def chain_early(i):
        @pl.when(jnp.logical_not(at_end))
        def _():
            chain_step(early, i)

    early = jnp.where(z < sp // 2, 0, 1)
    late = 1 - early
    at_end = (z == 0) | (z == sp - 1)

    def pair_stage(g):
        lanes = slice(g * GW, (g + 1) * GW)
        pb = mm(nrm[...], proj[:, pcol(g)], NN).astype(bf16).astype(f32)
        for i in range(2):
            k = 2 * g + i
            at = slice(k * LANES, (k + 1) * LANES)
            pairx[k] = pb[:, i * LANES : (i + 1) * LANES]
            act, slope = silu_parts(conv(pairx, k, tap_p, at))
            bc[k] = act.astype(bf16)
            bct[k] = act.T.astype(bf16)
            slp[k] = slope

        @pl.when(at_end)
        def _():
            for i in range(g * chunks, (g + 1) * chunks):
                at = slice(i * CW, (i + 1) * CW)
                cout[early, :, at] = mm(bct[2 * g + early], tx[early, :, at], NN).astype(bf16)

                @pl.when(has_out(early))
                def _():
                    go_state(early, i).start()

        @pl.when(jnp.logical_not(at_end))
        def _():
            for q in range(2):
                car[q, :, lanes] = mm(bct[2 * g + q], tx[q, :, lanes], NN)

        gm[g] = mm(bc[2 * g + 1], bct[2 * g], NN)

    def local_mix(g):
        gmat = gm[g]
        for j in range(g * tiles, (g + 1) * tiles):
            at = slice(j * LANES, (j + 1) * LANES)
            mixes = [(gmat * dec[2 * j + q]).astype(bf16) for q in range(2)]
            ybuf[:, at] = mm(jnp.concatenate(mixes, axis=1), halves(xb[:, at]), NN)
            dxl[:, at] = mm(jnp.concatenate(mixes, axis=0), halves(cot[:, at]), TN)

    def go_next(kind, g):
        if kind == 0:
            part = slice(2 * g, 2 * g + 2)
            src, dst = dpb.at[part, EDGE : EDGE + NEXT, :], dpn.at[part]
        else:
            part = slice(g * tiles, (g + 1) * tiles)
            src, dst = dvb.at[part, 0:NEXT, :], dvb.at[part, T : T + NEXT, :]
        return remote(
            src,
            dst,
            nx_sem.at[0, kind, g],
            nx_sem.at[1, kind, g],
            {"sp": below},
        )

    def send_next(kind, g):
        @pl.when(z > 0)
        def _():
            go_next(kind, g).start()

    def take_next(kind, g):
        @pl.when(z < sp - 1)
        def _():
            go_next(kind, g).wait_recv()

    def piece(g, q):
        return 2 * g + 1 - q

    def lanes_of(k):
        return pl.ds(pl.multiple_of(k * LANES, LANES), LANES)

    def pair_grads(g, q):
        lanes = slice(g * GW, (g + 1) * GW)
        k = piece(g, q)
        part = mm(dgs[g, q], bc[2 * g + q], NN) + mm(tx[1 - q, :, lanes], cin[q, :, lanes], NT)
        dpb[k, EDGE : EDGE + T, :] = part * slp[k]
        at = lanes_of(k)
        dpall[sent_rows(d), at] = conv_back(dpb, k, tap_p, at, 0, EDGE + T).astype(bf16)
        spread_out(go_dpair(k), dg_send.at[k])

    def go_dpair(k):
        def go(s, to, ss):
            at = dpall.at[sent_rows(s), lanes_of(k)]
            return remote(at, at, ss, dg_recv.at[k, s], {"dp": to})

        return go

    def pair_back(g):
        take_next(0, g)
        for k in range(2 * g, 2 * g + 2):
            at = slice(k * LANES, (k + 1) * LANES)
            dpb[k, EDGE + T : EDGE + T + NEXT, :] = dpn[k]
            dpair[:, at] = conv_back(dpb, k, tap_p, at, EDGE).astype(bf16)

    def value_grads(g):
        b = bc[2 * g]
        cc = bc[2 * g + 1]
        for j in range(g * tiles, (g + 1) * tiles):
            at = slice(j * LANES, (j + 1) * LANES)
            s_in = cin[0, :, at]
            ds = cin[1, :, at]
            dyf = cot[:, at].astype(f32)
            u = us[:, at]
            y = ybuf[:, at] + spread(ea, j) * mm(cc, s_in, NN)
            zbuf[0, 0:T, at] = dyf * y
            ybf = (y + spread(skips, j) * u).astype(bf16)
            gg[:, at] = (upslope[:, at] * ybf.astype(f32)).astype(bf16)
            x = xb[:, at].astype(f32)
            tej = spread(te, j)
            far = mm(b, ds, NN)
            dx = dxl[:, at] + tej * far
            zbuf[1, 0:T, at] = x * dx
            ends = jnp.sum(x * tej * far, axis=0, keepdims=True) + ee[:, at] * jnp.sum(
                ds.astype(f32) * s_in.astype(f32), axis=0, keepdims=True
            )
            zbuf[1, T : T + NEXT, at] = jnp.broadcast_to(ends, (NEXT, LANES))
            du = spread(dt, j) * dx + spread(skips, j) * dyf
            dvb[j, 0:T, :] = du * slv[:, at]
        send_next(1, g)

    def value_back(g):
        take_next(1, g)
        for j in range(g * tiles, (g + 1) * tiles):
            at = slice(j * LANES, (j + 1) * LANES)
            gv[:, at] = conv_back(dvb, j, tap_v, at).astype(bf16)

    def step_grads():
        sel_r = lax.broadcasted_iota(jnp.int32, (LANES, W), 0)
        sel_c = lax.broadcasted_iota(jnp.int32, (LANES, W), 1)
        sel = jnp.where(sel_c // HEAD == sel_r, 1.0, 0.0).astype(bf16)
        r1 = mm_split(zbuf[0, 0:T, :], sel, NT)
        both = mm_split(zbuf[1], sel, NT)
        xd = both[0:T]
        d_end = both[T : T + 1]
        back = mm_exact(tri, r1 - xd, TN) + d_end
        d_dt = (xd / dt + rate * back) * sgs
        gs[...] = d_dt.T[0:heads, :].astype(bf16)

    def go_nt(to):
        return remote(
            nt.at[prow(to), :], ntall.at[:, twice(d)], nt_send.at[to], nt_recv.at[d], {"dp": to}
        )

    def nt_from(s):
        return remote(nt.at[prow(d), :], ntall.at[:, twice(s)], nt_send.at[s], nt_recv.at[s], {"dp": s})

    def send_normed():
        for k in range(width // LANES):
            at = slice(k * LANES, (k + 1) * LANES)
            nt[at, T : 2 * T] = nrm[EDGE : EDGE + T, at].T
            edge = jnp.concatenate([jnp.zeros((T - EDGE, LANES), bf16), nrm[0:EDGE, at]], axis=0)
            nt[at, 0:T] = edge.T
        for off in range(1, dp):
            go_nt(lax.rem(d + off, dp)).start()
        ntall[:, twice(d)] = nt[prow(d), :]

    def row_part(p, i):
        return slice(i * (R // cuts), (i + 1) * (R // cuts)), lanes_of(p)

    def go_rows(q, p, i):
        r, c = row_part(p, i)
        k = p * cuts + i
        return remote(
            gout.at[q, r, c], gin.at[q, r, c], gc_send.at[q, k], gc_recv.at[q, k], {"sp": onward(q)}
        )

    def rows_step(q, p):
        for i in range(cuts):
            r, c = row_part(p, i)

            @pl.when(has_in(q))
            def _():
                go_rows(q, p, i).wait_recv()

            @pl.when(has_out(q))
            def _():
                gout[q, r, c] = (gin[q, r, c].astype(f32) + gpl[r, c]).astype(bf16)
                go_rows(q, p, i).start()

    def rows_ends(p):
        @pl.when(at_end)
        def _():
            rows_step(early, p)

    def rows_early(p):
        @pl.when(jnp.logical_not(at_end))
        def _():
            rows_step(early, p)

    def take_normed():
        for s in range(1, dp):
            nt_from(lax.rem(d + s, dp)).wait_recv()

    def rows_of(p):
        pass_on(go_dpair(p), dg_send.at[p], dg_relay.at[p])
        take_rest(go_dpair(p), dg_relay.at[p])
        at = lanes_of(p)
        gpl[:, at] = mm(ntall[...], dpall[:, at], NN)
        rows_ends(p)

    def rows_total(g):
        at = pcol(g)
        gp[:, at] = gin[0, :, at].astype(f32) + gpl[:, at] + gin[1, :, at].astype(f32)

    def pass_proj(g):
        pass_on(proj_of(g), pj_send.at[g], pj_relay.at[g])
        take_rest(proj_of(g), pj_relay.at[g])

    loads[1].wait()
    loads[2].wait()
    loads[3].wait()

    @pl.when(z > 0)
    def _():
        go_edge(0).wait_recv()

    for g in range(groups):
        before_pair(g)
    loads[4].wait()

    @pl.when(z > 0)
    def _():
        go_edge(1).wait_recv()

    pass_proj(0)
    pair_stage(0)
    local_mix(0)
    send_normed()
    done_early = 0
    for g in range(1, groups):
        pass_on(proj_of(g), pj_send.at[g], pj_relay.at[g])
        for _ in range(chunks // 4):
            chain_early(done_early)
            done_early += 1
        take_rest(proj_of(g), pj_relay.at[g])
        pair_stage(g)

    order = [(i, 0, i) for i in range(done_early, groups * chunks)]
    order += [(i + chunks // 2 + 0.5, 1, i) for i in range(groups * chunks)]
    for _, kind, i in sorted(order):
        g = i // chunks
        ends_group = (i + 1) % chunks == 0
        if kind == 0:
            chain_early(i)
            if ends_group:
                pair_grads(g, early)
        else:
            chain_step(late, i)
            if g > 0 and i % chunks == chunks // 2:
                if g == 1:
                    take_normed()
                rows_of(piece(g - 1, early))
            if ends_group:
                pair_grads(g, late)
                send_next(0, g)
                if g + 1 < groups:
                    local_mix(g + 1)

    tail = groups - 1
    for g in range(tail):
        rows_of(piece(g, late))
    rows_of(piece(tail, early))
    for g in range(tail):
        rows_early(piece(g, early))
        value_grads(g)
    rows_of(piece(tail, late))
    value_grads(tail)
    for g in range(tail):
        rows_step(late, piece(g, late))
        rows_early(piece(g, late))
    rows_early(piece(tail, early))
    for g in range(groups):
        pair_back(g)
    for k in range(width // 512):
        at = slice(k * 512, (k + 1) * 512)
        gn[:, at] = mm(dpair[...], proj[at, :], NT).astype(bf16)
    for g in range(tail):
        rows_step(late, piece(g, early))
        rows_total(g)
    rows_early(piece(tail, late))
    rows_step(late, piece(tail, late))
    for g in range(groups):
        value_back(g)
    step_grads()
    rows_step(late, piece(tail, early))
    rows_total(tail)

    for g in range(groups):
        drain(proj_of(g), pj_send.at[g], pj_relay.at[g])
    for k in range(pieces):
        drain(go_dpair(k), dg_send.at[k], dg_relay.at[k])
    for off in range(1, dp):
        go_nt(lax.rem(d + off, dp)).wait_send()

    @pl.when(z < sp - 1)
    def _():
        go_edge(0).wait_send()
        go_edge(1).wait_send()

    @pl.when(z > 0)
    def _():
        for g in range(groups):
            go_next(0, g).wait_send()
            go_next(1, g).wait_send()

    for q in range(2):
        @pl.when(has_out(q))
        def _():
            for i in range(groups * chunks):
                go_state(q, i).wait_send()
            for k in range(pieces):
                for i in range(cuts):
                    go_rows(q, k, i).wait_send()


def place_kernel(*refs):
    sources, targets, sem = refs[0:5], refs[5:10], refs[10]
    copies = [pltpu.make_async_copy(sources[k], targets[k], sem.at[k]) for k in range(5)]
    for copy in copies:
        copy.start()
    for copy in copies:
        copy.wait()


def per_device(
    normed,
    values,
    gate_in,
    step_raw,
    upstream,
    proj_pair,
    conv_value,
    conv_pair,
    step_bias,
    decay_log,
    skip,
):
    sp = lax.axis_size("sp")
    dp = lax.axis_size("dp")
    T = normed.shape[1]
    width = normed.shape[2]
    W = values.shape[2]
    heads = step_raw.shape[2]
    cols = proj_pair.shape[1]
    groups = cols // PAIR
    R = proj_pair.shape[0]
    chunks = min(8, W // groups // LANES)
    cuts = 4
    vmem = pl.BlockSpec(memory_space=pltpu.VMEM)
    hbm = pl.BlockSpec(memory_space=pltpu.HBM)
    V = pltpu.VMEM
    dma = pltpu.SemaphoreType.DMA
    vt = W // LANES
    pt = cols // LANES
    scratch = [
        V((heads, T), bf16),
        V((4, W), f32),
        V((4, cols), f32),
        V((1, heads), f32),
        V((1, heads), f32),
        V((1, heads), f32),
        V((EDGE + T, width), bf16),
        V((EDGE + T, W), bf16),
        V((T, W), bf16),
        V((T, W), bf16),
        V((width, cols), bf16),
        V((width, 2 * T), bf16),
        V((R, dp * 2 * T), bf16),
        V((T, W), bf16),
        V((vt, EDGE + T, LANES), f32),
        V((T, W), f32),
        V((T, W), f32),
        V((T, W), f32),
        V((T, W), bf16),
        V((2, T, W), bf16),
        V((heads, T, T), f32),
        V((groups, 2, T, T), bf16),
        V((groups, T, T), f32),
        V((pt, EDGE + T, LANES), f32),
        V((pt, T, LANES), bf16),
        V((pt, LANES, T), bf16),
        V((pt, T, LANES), f32),
        V((1, W), f32),
        V((2, STATE, W), f32),
        V((2, STATE, W), bf16),
        V((2, STATE, W), bf16),
        V((T, W), f32),
        V((T, W), f32),
        V((2, T + NEXT, W), f32),
        V((vt, T + NEXT, LANES), f32),
        V((pt, EDGE + T + NEXT, LANES), f32),
        V((pt, NEXT, LANES), f32),
        V((T, cols), bf16),
        V((dp * 2 * T, cols), bf16),
        V((R, cols), f32),
        V((2, R, cols), bf16),
        V((2, R, cols), bf16),
        dma((11,)),
        dma((2, 2)),
        dma((groups, dp)),
        dma((groups, dp)),
        dma((groups, dp)),
        dma((2, groups * chunks)),
        dma((2, groups * chunks)),
        dma((2, 2, groups)),
        dma((dp,)),
        dma((dp,)),
        dma((pt, dp)),
        dma((pt, dp)),
        dma((pt, dp)),
        dma((2, pt * cuts)),
        dma((2, pt * cuts)),
    ]
    gn, gv, gg, gs, gp = pl.pallas_call(
        functools.partial(mixer_kernel, sp, dp, heads, groups, chunks, cuts),
        out_shape=(
            jax.ShapeDtypeStruct((T, width), bf16),
            jax.ShapeDtypeStruct((T, W), bf16),
            jax.ShapeDtypeStruct((T, W), bf16),
            jax.ShapeDtypeStruct((heads, T), bf16),
            jax.ShapeDtypeStruct((R, cols), f32),
        ),
        in_specs=[hbm] * 11,
        out_specs=(vmem,) * 5,
        scratch_shapes=scratch,
        compiler_params=pltpu.CompilerParams(
            collective_id=0, has_side_effects=True, vmem_limit_bytes=40 * 1024 * 1024
        ),
    )(
        *[
            pltpu.with_memory_space_constraint(x, pltpu.HBM)
            for x in (
                normed[0],
                values[0],
                gate_in[0],
                upstream[0],
                proj_pair,
                step_raw[0].T,
                conv_value,
                conv_pair,
                step_bias[None],
                decay_log[None],
                skip[None],
            )
        ]
    )
    results = (gn, gv, gg, gs, gp)
    gn, gv, gg, gs, gp = pl.pallas_call(
        place_kernel,
        out_shape=tuple(jax.ShapeDtypeStruct(r.shape, r.dtype) for r in results),
        in_specs=[vmem] * 5,
        out_specs=(hbm,) * 5,
        scratch_shapes=[dma((5,))],
        compiler_params=pltpu.CompilerParams(vmem_limit_bytes=8 * 1024 * 1024),
    )(*results)
    return (gn[None], gv[None], gg[None], gs.T[None], gp)


def solution(mesh):
    tok = P("dp", "sp", None)
    in_specs = (tok, tok, tok, tok, tok, P("dp", None), P(), P(), P(), P(), P())
    out_specs = (tok, tok, tok, tok, P("dp", None))
    return jax.shard_map(
        per_device, mesh=mesh, in_specs=in_specs, out_specs=out_specs, check_vma=False
    )
```

```python
import functools

import jax
import jax.numpy as jnp
from jax import lax
from jax.experimental import pallas as pl
from jax.experimental.pallas import tpu as pltpu
from jax.sharding import PartitionSpec as P

HEAD = 64
STATE = 128
LANES = 128
PAIR = 2 * STATE
EDGE = 16
NEXT = 8
exact = lax.Precision.HIGHEST
f32 = jnp.float32
bf16 = jnp.bfloat16

NN = (((1,), (0,)), ((), ()))
NT = (((1,), (1,)), ((), ()))
TN = (((0,), (0,)), ((), ()))


def mm(a, b, dims):
    return lax.dot_general(a, b, dims, preferred_element_type=f32)


def mm_exact(a, b, dims):
    return lax.dot_general(a, b, dims, precision=exact, preferred_element_type=f32)


def mm_split(a, b, dims):
    high = a.astype(bf16)
    low = (a - high.astype(f32)).astype(bf16)
    return mm(high, b, dims) + mm(low, b, dims)


def silu_parts(s):
    sig = jax.nn.sigmoid(s)
    return s * sig, sig * (1.0 + s * (1.0 - sig))


def mixer_kernel(
    sp,
    dp,
    heads,
    groups,
    chunks,
    cuts,
    normed_in,
    values_in,
    gate_in,
    up_in,
    proj_in,
    step_in,
    tap_v_in,
    tap_p_in,
    bias_in,
    log_rate_in,
    skip_in,
    gn,
    gv,
    gg,
    gs,
    gp,
    step,
    tap_v,
    tap_p,
    bias,
    log_rate,
    skip,
    nrm,
    val,
    gate,
    up,
    proj,
    nt,
    ntall,
    cot,
    xvb,
    us,
    slv,
    upslope,
    xb,
    tx,
    dec,
    dgs,
    gm,
    pairx,
    bc,
    bct,
    slp,
    ee,
    car,
    cin,
    cout,
    ybuf,
    dxl,
    zbuf,
    dvb,
    dpb,
    dpn,
    dpair,
    dpall,
    gpl,
    gin,
    gout,
    loc_sem,
    edge_sem,
    pj_send,
    pj_recv,
    pj_relay,
    ch_send,
    ch_recv,
    nx_sem,
    nt_send,
    nt_recv,
    dg_send,
    dg_recv,
    dg_relay,
    gc_send,
    gc_recv,
):
    z = lax.axis_index("sp")
    d = lax.axis_index("dp")
    T = cot.shape[0]
    W = cot.shape[1]
    width = nt.shape[0]
    R = proj_in.shape[0]
    GW = W // groups
    tiles = GW // LANES
    CW = GW // chunks
    nch = dp // 2
    core = lax.rem(d, 2)
    chip = d // 2
    sib = d + 1 - 2 * core
    first = z == 0
    last = z == sp - 1

    def remote(src, dst, ss, rs, to):
        return pltpu.make_async_remote_copy(
            src_ref=src,
            dst_ref=dst,
            send_sem=ss,
            recv_sem=rs,
            device_id=to,
            device_id_type=pl.DeviceIdType.MESH,
        )

    def prow(s):
        return pl.ds(pl.multiple_of(s * R, 16), R)

    def twice(s):
        return pl.ds(pl.multiple_of(s * 2 * T, LANES), 2 * T)

    def sent_rows(s):
        return pl.ds(pl.multiple_of(s * 2 * T + T - EDGE, EDGE), EDGE + T)

    def pcol(g):
        return slice(g * PAIR, (g + 1) * PAIR)

    below = lax.max(z - 1, 0)
    above = lax.min(z + 1, sp - 1)

    loads = [
        pltpu.make_async_copy(proj_in, proj.at[prow(d), :], loc_sem.at[0]),
        pltpu.make_async_copy(gate_in, gate, loc_sem.at[1]),
        pltpu.make_async_copy(up_in, up, loc_sem.at[2]),
        pltpu.make_async_copy(values_in, val.at[EDGE : EDGE + T, :], loc_sem.at[3]),
        pltpu.make_async_copy(normed_in, nrm.at[EDGE : EDGE + T, :], loc_sem.at[4]),
    ]
    small = [
        pltpu.make_async_copy(src, dst, loc_sem.at[5 + k])
        for k, (src, dst) in enumerate(
            (
                (step_in, step),
                (bias_in, bias),
                (log_rate_in, log_rate),
                (skip_in, skip),
                (tap_v_in, tap_v),
                (tap_p_in, tap_p),
            )
        )
    ]
    loads[0].start()
    for load in small + loads[1:]:
        load.start()

    barrier = pltpu.get_barrier_semaphore()
    for off in range(1, dp):
        pl.semaphore_signal(
            barrier,
            inc=1,
            device_id={"dp": lax.rem(d + off, dp)},
            device_id_type=pl.DeviceIdType.MESH,
        )

    @pl.when(z > 0)
    def _():
        pl.semaphore_signal(
            barrier, inc=1, device_id={"sp": below}, device_id_type=pl.DeviceIdType.MESH
        )

    @pl.when(z < sp - 1)
    def _():
        pl.semaphore_signal(
            barrier, inc=1, device_id={"sp": above}, device_id_type=pl.DeviceIdType.MESH
        )

    arrivals = dp - 1 + jnp.where(first, 0, 1) + jnp.where(last, 0, 1)
    pl.semaphore_wait(barrier, arrivals)

    def go_proj(g, s, to, ss):
        at = proj.at[prow(s), pcol(g)]
        return remote(at, at, ss, pj_recv.at[g, s], {"dp": to})

    def chip_peer(off):
        if nch & (nch - 1):
            return lax.rem(chip + off, nch) * 2 + core
        to = chip
        for bit in range(off.bit_length()):
            if off >> bit & 1:
                to = to + (1 - 2 * lax.rem(chip // 2**bit, 2)) * 2**bit
        return to * 2 + core

    far_first = sorted(range(1, nch), key=lambda off: (-bin(off).count("1"), off))

    def spread_out(go, send):
        for off in far_first:
            to = chip_peer(off)
            go(d, to, send.at[to]).start()
        go(d, sib, send.at[sib]).start()

    def pass_on(go, send, relay):
        for off in far_first:
            s = chip_peer(off)
            go(s, sib, relay.at[s]).wait_recv()
            go(s, sib, relay.at[s]).start()

    def take_rest(go, relay):
        go(sib, sib, relay.at[sib]).wait_recv()
        for off in range(1, nch):
            s = chip_peer(off) + 1 - 2 * core
            go(s, sib, relay.at[s]).wait_recv()

    def drain(go, send, relay):
        for off in range(1, nch):
            to = chip_peer(off)
            go(d, to, send.at[to]).wait_send()
            go(to, sib, relay.at[to]).wait_send()
        go(d, sib, send.at[sib]).wait_send()

    def proj_of(g):
        return lambda s, to, ss: go_proj(g, s, to, ss)

    loads[0].wait()
    spread_out(proj_of(0), pj_send.at[0])

    def go_edge(k):
        src = (values_in, normed_in)[k]
        dst = (val, nrm)[k]
        return remote(
            src.at[T - EDGE : T, :], dst.at[0:EDGE, :], edge_sem.at[0, k], edge_sem.at[1, k], {"sp": above}
        )

    @pl.when(z < sp - 1)
    def _():
        go_edge(0).start()
        go_edge(1).start()

    for g in range(1, groups):
        spread_out(proj_of(g), pj_send.at[g])

    pieces = dpb.shape[0]
    dpb[:, 0:EDGE, :] = jnp.zeros((pieces, EDGE, LANES), f32)
    dpb[:, EDGE + T : EDGE + T + NEXT, :] = jnp.zeros((pieces, NEXT, LANES), f32)
    for s in range(dp):
        dpall[s * 2 * T : s * 2 * T + T - EDGE, :] = jnp.zeros((T - EDGE, dpall.shape[1]), bf16)

    @pl.when(first)
    def _():
        val[0:EDGE, :] = jnp.zeros((EDGE, W), bf16)
        nrm[0:EDGE, :] = jnp.zeros((EDGE, width), bf16)
        cin[0] = jnp.zeros((STATE, W), bf16)
        gin[0] = jnp.zeros(gin.shape[1:], bf16)

    @pl.when(last)
    def _():
        cin[1] = jnp.zeros((STATE, W), bf16)
        gin[1] = jnp.zeros(gin.shape[1:], bf16)
        dvb[:, T : T + NEXT, :] = jnp.zeros((dvb.shape[0], NEXT, LANES), f32)
        dpn[...] = jnp.zeros(dpn.shape, f32)

    for load in small:
        load.wait()
    row_i = lax.broadcasted_iota(jnp.int32, (T, T), 0)
    col_i = lax.broadcasted_iota(jnp.int32, (T, T), 1)
    causal = row_i >= col_i
    tri = causal.astype(f32)
    lane = lax.broadcasted_iota(jnp.int32, (T, LANES), 1)
    low = lane < HEAD

    def padded(v):
        return jnp.concatenate([v, jnp.zeros((v.shape[0], LANES - heads), f32)], axis=1)

    def spread(x, j):
        a = x[:, 2 * j : 2 * j + 1]
        b = x[:, 2 * j + 1 : 2 * j + 2]
        mask = low if x.shape[0] == T else low[0 : x.shape[0]]
        return jnp.where(mask, a, b)

    rate = -jnp.exp(padded(log_rate[...]))
    skips = padded(skip[...])
    steps = jnp.concatenate([step[...].astype(f32), jnp.zeros((LANES - heads, T), f32)], axis=0)
    raw = steps.T + padded(bias[...])
    dt = jax.nn.softplus(raw)
    sgs = jax.nn.sigmoid(raw)
    ac = mm_exact(tri, dt * rate, NN)
    ac_t = ac.T
    ea = jnp.exp(ac)
    end = ac[T - 1 : T, :]
    te = jnp.exp(end - ac)
    e_end = jnp.exp(end)

    def halves(v):
        zero = jnp.zeros_like(v)
        return jnp.concatenate([jnp.where(low, v, zero), jnp.where(low, zero, v)], axis=0)

    def conv(buf, k, taps, at):
        total = taps[0:1, at] * buf[k, EDGE - 3 : EDGE - 3 + T, :]
        for i in range(1, 4):
            total = total + taps[i : i + 1, at] * buf[k, EDGE - 3 + i : EDGE - 3 + i + T, :]
        return total

    def conv_back(buf, k, taps, at, start=0, count=T):
        total = taps[3:4, at] * buf[k, start : start + count, :]
        for i in range(3):
            total = total + taps[i : i + 1, at] * buf[k, start + 3 - i : start + 3 - i + count, :]
        return total

    def before_pair(g):
        d_g = jnp.zeros((T, T), f32)
        for j in range(g * tiles, (g + 1) * tiles):
            at = slice(j * LANES, (j + 1) * LANES)
            v = gate[:, at].astype(f32)
            upf = up[:, at].astype(f32)
            act, slope = silu_parts(v)
            dy = (upf * act).astype(bf16)
            cot[:, at] = dy
            upslope[:, at] = upf * slope
            xvb[j] = val[:, at].astype(f32)
            u, slope = silu_parts(conv(xvb, j, tap_v, at))
            us[:, at] = u
            slv[:, at] = slope
            x = (u * spread(dt, j)).astype(bf16)
            xb[:, at] = x
            tx[0, :, at] = (x.astype(f32) * spread(te, j)).astype(bf16)
            tx[1, :, at] = (spread(ea, j) * dy.astype(f32)).astype(bf16)
            ee[:, at] = spread(e_end, j)
            d_mix = mm(halves(dy), x, NT)
            for q in range(2):
                h = 2 * j + q
                diff = ac[:, h : h + 1] - ac_t[h : h + 1, :]
                decay = jnp.exp(jnp.where(causal, diff, -1e30))
                dec[h] = decay
                d_g = d_g + d_mix[q * T : (q + 1) * T] * decay
        dgs[g, 0] = d_g.astype(bf16)
        dgs[g, 1] = d_g.T.astype(bf16)

    def has_in(q):
        return jnp.where(q == 0, z > 0, z < sp - 1)

    def has_out(q):
        return jnp.where(q == 0, z < sp - 1, z > 0)

    def onward(q):
        return lax.max(lax.min(z + 1 - 2 * q, sp - 1), 0)

    def go_state(q, i):
        lanes = slice(i * CW, (i + 1) * CW)
        return remote(
            cout.at[q, :, lanes], cin.at[q, :, lanes], ch_send.at[q, i], ch_recv.at[q, i], {"sp": onward(q)}
        )

    def chain_step(q, i):
        lanes = slice(i * CW, (i + 1) * CW)

        @pl.when(has_in(q))
        def _():
            go_state(q, i).wait_recv()

        @pl.when(has_out(q))
        def _():
            total = cin[q, :, lanes].astype(f32) * ee[0:1, lanes] + car[q, :, lanes]
            cout[q, :, lanes] = total.astype(bf16)
            go_state(q, i).start()

    def chain_early(i):
        @pl.when(jnp.logical_not(at_end))
        def _():
            chain_step(early, i)

    early = jnp.where(z < sp // 2, 0, 1)
    late = 1 - early
    at_end = (z == 0) | (z == sp - 1)

    def pair_stage(g):
        lanes = slice(g * GW, (g + 1) * GW)
        pb = mm(nrm[...], proj[:, pcol(g)], NN).astype(bf16).astype(f32)
        for i in range(2):
            k = 2 * g + i
            at = slice(k * LANES, (k + 1) * LANES)
            pairx[k] = pb[:, i * LANES : (i + 1) * LANES]
            act, slope = silu_parts(conv(pairx, k, tap_p, at))
            bc[k] = act.astype(bf16)
            bct[k] = act.T.astype(bf16)
            slp[k] = slope

        @pl.when(at_end)
        def _():
            for i in range(g * chunks, (g + 1) * chunks):
                at = slice(i * CW, (i + 1) * CW)
                cout[early, :, at] = mm(bct[2 * g + early], tx[early, :, at], NN).astype(bf16)

                @pl.when(has_out(early))
                def _():
                    go_state(early, i).start()

        @pl.when(jnp.logical_not(at_end))
        def _():
            for q in range(2):
                car[q, :, lanes] = mm(bct[2 * g + q], tx[q, :, lanes], NN)

        gm[g] = mm(bc[2 * g + 1], bct[2 * g], NN)

    def local_mix(g):
        gmat = gm[g]
        for j in range(g * tiles, (g + 1) * tiles):
            at = slice(j * LANES, (j + 1) * LANES)
            mixes = [(gmat * dec[2 * j + q]).astype(bf16) for q in range(2)]
            ybuf[:, at] = mm(jnp.concatenate(mixes, axis=1), halves(xb[:, at]), NN)
            dxl[:, at] = mm(jnp.concatenate(mixes, axis=0), halves(cot[:, at]), TN)

    def go_next(kind, g):
        if kind == 0:
            part = slice(2 * g, 2 * g + 2)
            src, dst = dpb.at[part, EDGE : EDGE + NEXT, :], dpn.at[part]
        else:
            part = slice(g * tiles, (g + 1) * tiles)
            src, dst = dvb.at[part, 0:NEXT, :], dvb.at[part, T : T + NEXT, :]
        return remote(
            src,
            dst,
            nx_sem.at[0, kind, g],
            nx_sem.at[1, kind, g],
            {"sp": below},
        )

    def send_next(kind, g):
        @pl.when(z > 0)
        def _():
            go_next(kind, g).start()

    def take_next(kind, g):
        @pl.when(z < sp - 1)
        def _():
            go_next(kind, g).wait_recv()

    def piece(g, q):
        return 2 * g + 1 - q

    def lanes_of(k):
        return pl.ds(pl.multiple_of(k * LANES, LANES), LANES)

    def pair_grads(g, q):
        lanes = slice(g * GW, (g + 1) * GW)
        k = piece(g, q)
        part = mm(dgs[g, q], bc[2 * g + q], NN) + mm(tx[1 - q, :, lanes], cin[q, :, lanes], NT)
        dpb[k, EDGE : EDGE + T, :] = part * slp[k]
        at = lanes_of(k)
        dpall[sent_rows(d), at] = conv_back(dpb, k, tap_p, at, 0, EDGE + T).astype(bf16)
        spread_out(go_dpair(k), dg_send.at[k])

    def go_dpair(k):
        def go(s, to, ss):
            at = dpall.at[sent_rows(s), lanes_of(k)]
            return remote(at, at, ss, dg_recv.at[k, s], {"dp": to})

        return go

    def pair_back(g):
        take_next(0, g)
        for k in range(2 * g, 2 * g + 2):
            at = slice(k * LANES, (k + 1) * LANES)
            dpb[k, EDGE + T : EDGE + T + NEXT, :] = dpn[k]
            dpair[:, at] = conv_back(dpb, k, tap_p, at, EDGE).astype(bf16)

    def value_grads(g):
        b = bc[2 * g]
        cc = bc[2 * g + 1]
        for j in range(g * tiles, (g + 1) * tiles):
            at = slice(j * LANES, (j + 1) * LANES)
            s_in = cin[0, :, at]
            ds = cin[1, :, at]
            dyf = cot[:, at].astype(f32)
            u = us[:, at]
            y = ybuf[:, at] + spread(ea, j) * mm(cc, s_in, NN)
            zbuf[0, 0:T, at] = dyf * y
            ybf = (y + spread(skips, j) * u).astype(bf16)
            gg[:, at] = (upslope[:, at] * ybf.astype(f32)).astype(bf16)
            x = xb[:, at].astype(f32)
            tej = spread(te, j)
            far = mm(b, ds, NN)
            dx = dxl[:, at] + tej * far
            zbuf[1, 0:T, at] = x * dx
            ends = jnp.sum(x * tej * far, axis=0, keepdims=True) + ee[:, at] * jnp.sum(
                ds.astype(f32) * s_in.astype(f32), axis=0, keepdims=True
            )
            zbuf[1, T : T + NEXT, at] = jnp.broadcast_to(ends, (NEXT, LANES))
            du = spread(dt, j) * dx + spread(skips, j) * dyf
            dvb[j, 0:T, :] = du * slv[:, at]
        send_next(1, g)

    def value_back(g):
        take_next(1, g)
        for j in range(g * tiles, (g + 1) * tiles):
            at = slice(j * LANES, (j + 1) * LANES)
            gv[:, at] = conv_back(dvb, j, tap_v, at).astype(bf16)

    def step_grads():
        sel_r = lax.broadcasted_iota(jnp.int32, (LANES, W), 0)
        sel_c = lax.broadcasted_iota(jnp.int32, (LANES, W), 1)
        sel = jnp.where(sel_c // HEAD == sel_r, 1.0, 0.0).astype(bf16)
        r1 = mm_split(zbuf[0, 0:T, :], sel, NT)
        both = mm_split(zbuf[1], sel, NT)
        xd = both[0:T]
        d_end = both[T : T + 1]
        back = mm_exact(tri, r1 - xd, TN) + d_end
        d_dt = (xd / dt + rate * back) * sgs
        gs[...] = d_dt.T[0:heads, :].astype(bf16)

    def go_nt(to):
        return remote(
            nt.at[prow(to), :], ntall.at[:, twice(d)], nt_send.at[to], nt_recv.at[d], {"dp": to}
        )

    def nt_from(s):
        return remote(nt.at[prow(d), :], ntall.at[:, twice(s)], nt_send.at[s], nt_recv.at[s], {"dp": s})

    def send_normed():
        for k in range(width // LANES):
            at = slice(k * LANES, (k + 1) * LANES)
            nt[at, T : 2 * T] = nrm[EDGE : EDGE + T, at].T
            edge = jnp.concatenate([jnp.zeros((T - EDGE, LANES), bf16), nrm[0:EDGE, at]], axis=0)
            nt[at, 0:T] = edge.T
        for off in range(1, dp):
            go_nt(lax.rem(d + off, dp)).start()
        ntall[:, twice(d)] = nt[prow(d), :]

    def row_part(p, i):
        return slice(i * (R // cuts), (i + 1) * (R // cuts)), lanes_of(p)

    def go_rows(q, p, i):
        r, c = row_part(p, i)
        k = p * cuts + i
        return remote(
            gout.at[q, r, c], gin.at[q, r, c], gc_send.at[q, k], gc_recv.at[q, k], {"sp": onward(q)}
        )

    def rows_step(q, p):
        for i in range(cuts):
            r, c = row_part(p, i)

            @pl.when(has_in(q))
            def _():
                go_rows(q, p, i).wait_recv()

            @pl.when(has_out(q))
            def _():
                gout[q, r, c] = (gin[q, r, c].astype(f32) + gpl[r, c]).astype(bf16)
                go_rows(q, p, i).start()

    def rows_ends(p):
        @pl.when(at_end)
        def _():
            rows_step(early, p)

    def rows_early(p):
        @pl.when(jnp.logical_not(at_end))
        def _():
            rows_step(early, p)

    def take_normed():
        for s in range(1, dp):
            nt_from(lax.rem(d + s, dp)).wait_recv()

    def rows_of(p):
        pass_on(go_dpair(p), dg_send.at[p], dg_relay.at[p])
        take_rest(go_dpair(p), dg_relay.at[p])
        at = lanes_of(p)
        gpl[:, at] = mm(ntall[...], dpall[:, at], NN)
        rows_ends(p)

    def rows_total(g):
        at = pcol(g)
        gp[:, at] = gin[0, :, at].astype(f32) + gpl[:, at] + gin[1, :, at].astype(f32)

    def pass_proj(g):
        pass_on(proj_of(g), pj_send.at[g], pj_relay.at[g])
        take_rest(proj_of(g), pj_relay.at[g])

    loads[1].wait()
    loads[2].wait()
    loads[3].wait()

    @pl.when(z > 0)
    def _():
        go_edge(0).wait_recv()

    for g in range(groups):
        before_pair(g)
    loads[4].wait()

    @pl.when(z > 0)
    def _():
        go_edge(1).wait_recv()

    pass_proj(0)
    pair_stage(0)
    local_mix(0)
    send_normed()
    done_early = 0
    for g in range(1, groups):
        pass_on(proj_of(g), pj_send.at[g], pj_relay.at[g])
        for _ in range(chunks // 4):
            chain_early(done_early)
            done_early += 1
        take_rest(proj_of(g), pj_relay.at[g])
        pair_stage(g)

    order = [(i, 0, i) for i in range(done_early, groups * chunks)]
    order += [(i + chunks // 2 + 0.5, 1, i) for i in range(groups * chunks)]
    for _, kind, i in sorted(order):
        g = i // chunks
        ends_group = (i + 1) % chunks == 0
        if kind == 0:
            chain_early(i)
            if ends_group:
                pair_grads(g, early)
        else:
            chain_step(late, i)
            if g > 0 and i % chunks == chunks // 2:
                if g == 1:
                    take_normed()
                rows_of(piece(g - 1, early))
            if ends_group:
                pair_grads(g, late)
                send_next(0, g)
                if g + 1 < groups:
                    local_mix(g + 1)

    tail = groups - 1
    for g in range(tail):
        rows_of(piece(g, late))
    rows_of(piece(tail, early))
    for g in range(tail):
        rows_early(piece(g, early))
        value_grads(g)
    rows_of(piece(tail, late))
    value_grads(tail)
    for g in range(tail):
        rows_step(late, piece(g, late))
        rows_early(piece(g, late))
    rows_early(piece(tail, early))
    for g in range(groups):
        pair_back(g)
    for k in range(width // 512):
        at = slice(k * 512, (k + 1) * 512)
        gn[:, at] = mm(dpair[...], proj[at, :], NT).astype(bf16)
    for g in range(tail):
        rows_step(late, piece(g, early))
        rows_total(g)
    rows_early(piece(tail, late))
    rows_step(late, piece(tail, late))
    for g in range(groups):
        value_back(g)
    step_grads()
    rows_step(late, piece(tail, early))
    rows_total(tail)

    for g in range(groups):
        drain(proj_of(g), pj_send.at[g], pj_relay.at[g])
    for k in range(pieces):
        drain(go_dpair(k), dg_send.at[k], dg_relay.at[k])
    for off in range(1, dp):
        go_nt(lax.rem(d + off, dp)).wait_send()

    @pl.when(z < sp - 1)
    def _():
        go_edge(0).wait_send()
        go_edge(1).wait_send()

    @pl.when(z > 0)
    def _():
        for g in range(groups):
            go_next(0, g).wait_send()
            go_next(1, g).wait_send()

    for q in range(2):
        @pl.when(has_out(q))
        def _():
            for i in range(groups * chunks):
                go_state(q, i).wait_send()
            for k in range(pieces):
                for i in range(cuts):
                    go_rows(q, k, i).wait_send()


def place_kernel(parts, *refs):
    sources, targets, sem = refs[0:5], refs[5:10], refs[10]
    copies = []
    for k in range(5):
        rows = sources[k].shape[0]
        count = parts if rows % (16 * parts) == 0 else 1
        for i in range(count):
            at = slice(i * (rows // count), (i + 1) * (rows // count))
            copies.append(
                pltpu.make_async_copy(sources[k].at[at, :], targets[k].at[at, :], sem.at[k, i])
            )
    for copy in copies:
        copy.start()
    for copy in copies:
        copy.wait()


def per_device(
    normed,
    values,
    gate_in,
    step_raw,
    upstream,
    proj_pair,
    conv_value,
    conv_pair,
    step_bias,
    decay_log,
    skip,
):
    sp = lax.axis_size("sp")
    dp = lax.axis_size("dp")
    T = normed.shape[1]
    width = normed.shape[2]
    W = values.shape[2]
    heads = step_raw.shape[2]
    cols = proj_pair.shape[1]
    groups = cols // PAIR
    R = proj_pair.shape[0]
    chunks = min(8, W // groups // LANES)
    cuts = 4
    vmem = pl.BlockSpec(memory_space=pltpu.VMEM)
    hbm = pl.BlockSpec(memory_space=pltpu.HBM)
    V = pltpu.VMEM
    dma = pltpu.SemaphoreType.DMA
    vt = W // LANES
    pt = cols // LANES
    scratch = [
        V((heads, T), bf16),
        V((4, W), f32),
        V((4, cols), f32),
        V((1, heads), f32),
        V((1, heads), f32),
        V((1, heads), f32),
        V((EDGE + T, width), bf16),
        V((EDGE + T, W), bf16),
        V((T, W), bf16),
        V((T, W), bf16),
        V((width, cols), bf16),
        V((width, 2 * T), bf16),
        V((R, dp * 2 * T), bf16),
        V((T, W), bf16),
        V((vt, EDGE + T, LANES), f32),
        V((T, W), f32),
        V((T, W), f32),
        V((T, W), f32),
        V((T, W), bf16),
        V((2, T, W), bf16),
        V((heads, T, T), f32),
        V((groups, 2, T, T), bf16),
        V((groups, T, T), f32),
        V((pt, EDGE + T, LANES), f32),
        V((pt, T, LANES), bf16),
        V((pt, LANES, T), bf16),
        V((pt, T, LANES), f32),
        V((1, W), f32),
        V((2, STATE, W), f32),
        V((2, STATE, W), bf16),
        V((2, STATE, W), bf16),
        V((T, W), f32),
        V((T, W), f32),
        V((2, T + NEXT, W), f32),
        V((vt, T + NEXT, LANES), f32),
        V((pt, EDGE + T + NEXT, LANES), f32),
        V((pt, NEXT, LANES), f32),
        V((T, cols), bf16),
        V((dp * 2 * T, cols), bf16),
        V((R, cols), f32),
        V((2, R, cols), bf16),
        V((2, R, cols), bf16),
        dma((11,)),
        dma((2, 2)),
        dma((groups, dp)),
        dma((groups, dp)),
        dma((groups, dp)),
        dma((2, groups * chunks)),
        dma((2, groups * chunks)),
        dma((2, 2, groups)),
        dma((dp,)),
        dma((dp,)),
        dma((pt, dp)),
        dma((pt, dp)),
        dma((pt, dp)),
        dma((2, pt * cuts)),
        dma((2, pt * cuts)),
    ]
    gn, gv, gg, gs, gp = pl.pallas_call(
        functools.partial(mixer_kernel, sp, dp, heads, groups, chunks, cuts),
        out_shape=(
            jax.ShapeDtypeStruct((T, width), bf16),
            jax.ShapeDtypeStruct((T, W), bf16),
            jax.ShapeDtypeStruct((T, W), bf16),
            jax.ShapeDtypeStruct((heads, T), bf16),
            jax.ShapeDtypeStruct((R, cols), f32),
        ),
        in_specs=[hbm] * 11,
        out_specs=(vmem,) * 5,
        scratch_shapes=scratch,
        compiler_params=pltpu.CompilerParams(
            collective_id=0, has_side_effects=True, vmem_limit_bytes=40 * 1024 * 1024
        ),
    )(
        *[
            pltpu.with_memory_space_constraint(x, pltpu.HBM)
            for x in (
                normed[0],
                values[0],
                gate_in[0],
                upstream[0],
                proj_pair,
                step_raw[0].T,
                conv_value,
                conv_pair,
                step_bias[None],
                decay_log[None],
                skip[None],
            )
        ]
    )
    results = (gn, gv, gg, gs, gp)
    gn, gv, gg, gs, gp = pl.pallas_call(
        functools.partial(place_kernel, 4),
        out_shape=tuple(jax.ShapeDtypeStruct(r.shape, r.dtype) for r in results),
        in_specs=[vmem] * 5,
        out_specs=(hbm,) * 5,
        scratch_shapes=[dma((5, 4))],
        compiler_params=pltpu.CompilerParams(vmem_limit_bytes=8 * 1024 * 1024),
    )(*results)
    return (gn[None], gv[None], gg[None], gs.T[None], gp)


def solution(mesh):
    tok = P("dp", "sp", None)
    in_specs = (tok, tok, tok, tok, tok, P("dp", None), P(), P(), P(), P(), P())
    out_specs = (tok, tok, tok, tok, P("dp", None))
    return jax.shard_map(
        per_device, mesh=mesh, in_specs=in_specs, out_specs=out_specs, check_vma=False
    )
```
